256 devices in a mesh: tp: 32 (over z, y), dp: 8 (over x, core).
Axes of the slice: x: 4, y: 4, z: 8, core: 2. Of those that a mesh axis runs over, the one named last changes fastest.
Arguments:
- stream: bfloat16 [256, 2048], P('tp', 'dp'), may hold values from -12 to 12
- norm_gain: float32 [2, 2048], P(None, 'dp'), may hold values from 0.1 to 1.9
- w_input: bfloat16 [2, 2048, 2048], P(None, 'dp', 'tp'), may hold values from -0.125 to 0.125
- lam_re: float32 [2, 128, 64], P(None, 'tp'), may hold values from -1 to -0.05
- lam_im: float32 [2, 128, 64], P(None, 'tp'), may hold values from 0 to 6
- log_dt: float32 [2, 128], P(None, 'tp'), may hold values from -3 to 0
- b_re: float32 [2, 128, 64, 16], P(None, 'tp'), may hold values from -1 to 1
- b_im: float32 [2, 128, 64, 16], P(None, 'tp'), may hold values from -1 to 1
- readout_real: float32 [2, 128, 16, 64], P(None, 'tp'), may hold values from -0.5 to 0.5
- readout_imaginary: float32 [2, 128, 16, 64], P(None, 'tp'), may hold values from -0.5 to 0.5
- d_skip: float32 [2, 2048], P(None, 'tp'), may hold values from -4 to 4
- w_val: bfloat16 [2, 2048, 2048], P(None, 'tp', 'dp'), may hold values from -0.375 to 0.375
- w_gate: bfloat16 [2, 2048, 2048], P(None, 'tp', 'dp'), may hold values from -0.375 to 0.375
- state: float32 [2, 256, 128, 128], P(None, 'dp', 'tp'), may hold values from -6 to 6
Outputs:
- stream_out: bfloat16 [256, 2048], P('tp', 'dp')
- states_out: float32 [2, 256, 128, 128], P(None, 'dp', 'tp')
The draws below stay inside these ranges and needn't reach their ends.
All inputs are finite; a program needn't handle non-finite values.
Results may differ from the reference program's by a relative error of at most 0.0064.
Values may be sent and summed in bfloat16 or wider, within the bound.
No kernel may reach another device: no remote copies, remote signals or barrier semaphores. Data moves between devices by JAX's collectives and lax.ppermute only.
A program may use at most 64 MiB of HBM per device.

```python
import jax
import jax.numpy as jnp
from jax import lax

D = 2048
CH = 16
STATE = 64
GROUPS = 128
LAYERS = 2
SEQS = 256


def draw_stream(key, part):
    subkeys = jax.random.split(key, 2)
    base_draw = jax.random.normal(subkeys[0], (SEQS, D), jnp.float32)
    block_scale = jnp.exp(jax.random.uniform(subkeys[1], (SEQS, 8), jnp.float32, -1.2, 1.2))
    full_draw = base_draw * jnp.repeat(block_scale, D // 8, axis=1)
    return jnp.clip(full_draw, -12.0, 12.0).astype(jnp.bfloat16)


def level_of(rng, extent, cuts, low, largest):
    loudness, own = 1.0, jax.random.fold_in(rng, 6)
    for dim, shards_of in cuts:
        heights = jnp.exp(jax.random.uniform(jax.random.fold_in(own, dim), (shards_of,), jnp.float32, low / len(cuts), largest / len(cuts)))
        loudness = loudness * jnp.repeat(heights, extent[dim] // shards_of).reshape([-1 if axis == dim else 1 for axis in range(len(extent))])
    return loudness


def bell_draw(rng, shape, scale, limit, cuts=(), held_as=jnp.bfloat16):
    result = scale * jax.random.normal(rng, shape, jnp.float32)
    if cuts:
        result = result * level_of(rng, shape, cuts, -0.22, 0.18)
    return jnp.clip(result, -limit, limit).astype(held_as)


def setup_inputs(seed: int = 0) -> dict:
    keys = jax.random.split(jax.random.key(seed), 15)
    stream = draw_stream(jax.random.fold_in(keys[14], 71), 0)
    norm_gain = jnp.clip(1.0 + 0.18 * jax.random.normal(keys[1], (LAYERS, D), jnp.float32), 0.1, 1.9)
    w_input = bell_draw(keys[2], (LAYERS, D, D), D ** -0.5, 0.125, ((1, 8), (2, 32)))
    lam_re = jnp.clip(-1.0 + 0.95 * jax.random.uniform(keys[3], (LAYERS, GROUPS, STATE), jnp.float32) ** level_of(keys[3], (LAYERS, GROUPS, STATE), ((1, 32),), -0.2, 0.2), -1.0, -0.05)
    lam_im = jnp.clip(6.0 * jax.random.uniform(keys[4], (LAYERS, GROUPS, STATE), jnp.float32) ** level_of(keys[4], (LAYERS, GROUPS, STATE), ((1, 32),), -0.2, 0.2), 0.0, 6.0)
    log_dt = jnp.clip(-3.0 + 3.0 * jax.random.uniform(keys[5], (LAYERS, GROUPS), jnp.float32) ** level_of(keys[5], (LAYERS, GROUPS), ((1, 32),), -0.2, 0.2), -3.0, 0.0)
    b_re = bell_draw(keys[6], (LAYERS, GROUPS, STATE, CH), (2 * CH) ** -0.5, 1.0, ((1, 32),), jnp.float32)
    b_im = bell_draw(keys[7], (LAYERS, GROUPS, STATE, CH), (2 * CH) ** -0.5, 1.0, ((1, 32),), jnp.float32)
    readout_real = bell_draw(keys[8], (LAYERS, GROUPS, CH, STATE), (2 * STATE) ** -0.5, 0.5, ((1, 32),), jnp.float32)
    readout_imaginary = bell_draw(keys[9], (LAYERS, GROUPS, CH, STATE), (2 * STATE) ** -0.5, 0.5, ((1, 32),), jnp.float32)
    d_skip = bell_draw(keys[10], (LAYERS, D), 1.0, 4.0, ((1, 32),), jnp.float32)
    w_val = bell_draw(keys[11], (LAYERS, D, D), (D // 8) ** -0.5, 0.375, ((1, 32), (2, 8)))
    w_gate = bell_draw(keys[12], (LAYERS, D, D), (D // 8) ** -0.5, 0.375, ((1, 32), (2, 8)))
    state = bell_draw(keys[13], (LAYERS, SEQS, GROUPS, 2 * STATE), 1.0, 6.0, ((1, 8), (2, 32)), jnp.float32)
    return {"stream": stream, "norm_gain": norm_gain, "w_input": w_input, "lam_re": lam_re, "lam_im": lam_im, "log_dt": log_dt, "b_re": b_re, "b_im": b_im, "readout_real": readout_real, "readout_imaginary": readout_imaginary, "d_skip": d_skip, "w_val": w_val, "w_gate": w_gate, "state": state}


eps = 1e-06

def advance(inputs, old_state, lam_re, lam_im, log_dt, b_re, b_im, readout_real, readout_imaginary, d_skip):
    upper_bound = lax.Precision.HIGHEST
    count_rows, groups, doubled = old_state.shape
    half_state = doubled // 2
    chans = b_re.shape[-1]
    step_size = jnp.exp(log_dt)[:, None]
    decay = jnp.exp(lam_re * step_size)
    angle = lam_im * step_size
    keep_re = decay * jnp.cos(angle)
    keep_im = decay * jnp.sin(angle)
    denom = lam_re * lam_re + lam_im * lam_im
    ratio_re = ((keep_re - 1.0) * lam_re + keep_im * lam_im) / denom
    ratio_im = (keep_im * lam_re - (keep_re - 1.0) * lam_im) / denom
    drive_re = ratio_re[..., None] * b_re - ratio_im[..., None] * b_im
    drive_im = ratio_re[..., None] * b_im + ratio_im[..., None] * b_re
    grouped = inputs.reshape(count_rows, groups, chans)
    push_re = jnp.einsum('gpc,rgc->rgp', drive_re, grouped, precision=upper_bound)
    push_im = jnp.einsum('gpc,rgc->rgp', drive_im, grouped, precision=upper_bound)
    old_re = old_state[..., :half_state]
    old_im = old_state[..., half_state:]
    updated_real = keep_re * old_re - keep_im * old_im + push_re
    updated_imaginary = keep_re * old_im + keep_im * old_re + push_im
    readout_output = jnp.einsum('aot,mat->mao', readout_real, updated_real, precision=upper_bound) - jnp.einsum('aot,mat->mao', readout_imaginary, updated_imaginary, precision=upper_bound)
    pre_act = readout_output.reshape(count_rows, groups * chans) + d_skip * inputs
    return (pre_act, jnp.concatenate([updated_real, updated_imaginary], axis=-1))

def reference(stream, norm_gain, w_input, lam_re, lam_im, log_dt, b_re, b_im, readout_real, readout_imaginary, d_skip, w_val, w_gate, state):
    collected = []
    for layer_no in range(LAYERS):
        widened = stream.astype(jnp.float32)
        factor = lax.rsqrt(lax.optimization_barrier(jnp.mean(widened * widened, axis=1)) + eps)
        normed = (widened * norm_gain[layer_no]).astype(jnp.bfloat16)
        inputs = factor[:, None] * jnp.dot(normed, w_input[layer_no], preferred_element_type=jnp.float32)
        pre_act, new_state = advance(inputs, state[layer_no], lam_re[layer_no], lam_im[layer_no], log_dt[layer_no], b_re[layer_no], b_im[layer_no], readout_real[layer_no], readout_imaginary[layer_no], d_skip[layer_no])
        mixed = jax.nn.gelu(pre_act).astype(jnp.bfloat16)
        value = jnp.dot(mixed, w_val[layer_no], preferred_element_type=jnp.float32)
        gate = jnp.dot(mixed, w_gate[layer_no], preferred_element_type=jnp.float32)
        stream = (widened + value * jax.nn.sigmoid(gate)).astype(jnp.bfloat16)
        collected.append(new_state)
    return (stream, jnp.stack(collected))
```

```python
import jax
import jax.numpy as jnp
from jax import lax
from jax.sharding import Mesh
from jax.sharding import PartitionSpec as P

D = 2048
LAYERS = 2
NZ, NY, NX, NC = 8, 4, 4, 2
ND = NX * NC
TP = ("z", "y")
DP = ("x", "c")
ALL = ("z", "y", "x", "c")

eps = 1e-06
HIGHEST = lax.Precision.HIGHEST


def gather_z(block):
    return lax.all_to_all(jnp.broadcast_to(block[None], (NZ, *block.shape)), "z", 0, 0, tiled=True)


def spread_dp(block):
    return lax.all_to_all(jnp.broadcast_to(block[None], (ND, *block.shape)), DP, 0, 0, tiled=True)


def turn(value):
    pairs = []
    for z in range(NZ):
        for y in range(NY):
            for d in range(ND):
                pairs.append(((z * NY + y) * ND + d, (d * NY + y) * ND + z))
    return lax.ppermute(value, ALL, pairs)


def shift_y(value, k):
    return lax.ppermute(value, "y", [(i, (i + k) % NY) for i in range(NY)])


def two_halves(value):
    high = value.astype(jnp.bfloat16)
    low = (value - high.astype(jnp.float32)).astype(jnp.bfloat16)
    return high, low


def joined(high, low):
    return high.astype(jnp.float32) + low.astype(jnp.float32)


def prepare(old_state, lam_re, lam_im, log_dt, b_re, b_im, readout_real, readout_imaginary, d_skip):
    half = old_state.shape[-1] // 2
    step_size = jnp.exp(log_dt)[:, None]
    decay = jnp.exp(lam_re * step_size)
    angle = lam_im * step_size
    keep_re = decay * jnp.cos(angle)
    keep_im = decay * jnp.sin(angle)
    denom = lam_re * lam_re + lam_im * lam_im
    ratio_re = ((keep_re - 1.0) * lam_re + keep_im * lam_im) / denom
    ratio_im = (keep_im * lam_re - (keep_re - 1.0) * lam_im) / denom
    drive_re = ratio_re[..., None] * b_re - ratio_im[..., None] * b_im
    drive_im = ratio_re[..., None] * b_im + ratio_im[..., None] * b_re
    drive = jnp.concatenate([drive_re, drive_im], axis=1)
    read = jnp.concatenate([readout_real, -readout_imaginary], axis=2)
    old_re = old_state[..., :half]
    old_im = old_state[..., half:]
    base = jnp.concatenate(
        [keep_re * old_re - keep_im * old_im, keep_re * old_im + keep_im * old_re], axis=-1
    )
    groups, chans = read.shape[:2]
    offset = jnp.einsum("rgp,gop->rgo", base, read, precision=HIGHEST)
    offset = offset.reshape(offset.shape[0], groups * chans)
    inner = jnp.einsum("gpc,gop->gco", drive, read, precision=HIGHEST)
    eye = jnp.eye(groups, dtype=jnp.float32)
    mix = (inner[:, :, None, :] * eye[:, None, :, None]).reshape(groups * chans, groups * chans)
    mix = mix + jnp.eye(groups * chans, dtype=jnp.float32) * d_skip[None, :]
    return base, drive, offset, mix


def per_device(
    stream,
    norm_gain,
    w_input,
    lam_re,
    lam_im,
    log_dt,
    b_re,
    b_im,
    readout_real,
    readout_imaginary,
    d_skip,
    w_val,
    w_gate,
    state,
):
    y_index = lax.axis_index("y")
    d_index = lax.axis_index("x") * NC + lax.axis_index("c")
    w_in_turned = [gather_z(w_input[0].T), None]

    rows = stream.shape[0]
    cols = stream.shape[1]
    pieces = [stream] + [shift_y(stream, k) for k in range(1, NY)]
    stacked = jnp.stack(pieces)
    order = (y_index - jnp.arange(NY)) % NY
    hot = (order[:, None] == jnp.arange(NY)[None, :]).astype(jnp.bfloat16)
    wide = jnp.einsum("ky,krc->yrc", hot, stacked, preferred_element_type=jnp.float32)
    x = wide.reshape(NY * rows, cols)

    prepared = [
        prepare(
            state[n],
            lam_re[n],
            lam_im[n],
            log_dt[n],
            b_re[n],
            b_im[n],
            readout_real[n],
            readout_imaginary[n],
            d_skip[n],
        )
        for n in range(LAYERS)
    ]
    offsets = turn(jnp.stack([p[2] for p in prepared]))

    def out_weights(n):
        return jnp.concatenate([w_val[n], w_gate[n], *two_halves(prepared[n][3])], axis=1)

    late = [gather_z(out_weights(0)), None]
    w_in_turned[1] = gather_z(w_input[1].T)
    late[1] = gather_z(out_weights(1))

    seqs = x.shape[0]
    chans = w_input.shape[2]
    returned = []
    for n in range(LAYERS):
        normed = (x * norm_gain[n]).astype(jnp.bfloat16)
        squares = jnp.sum(x * x, axis=1)
        partial = lax.dot_general(
            normed,
            w_in_turned[n].reshape(NZ * chans, cols),
            (((1,), (1,)), ((), ())),
            preferred_element_type=jnp.float32,
        )
        s_high, s_low = two_halves(squares[:, None])
        pad = jnp.zeros((seqs, 126), jnp.bfloat16)
        o_high, o_low = two_halves(offsets[n])
        payload = jnp.concatenate(
            [partial.astype(jnp.bfloat16), o_high, o_low, s_high, s_low, pad], axis=1
        )
        got = spread_dp(payload).astype(jnp.float32)
        width = NZ * chans
        total = jnp.sum(got[:, :, :width], axis=0)
        offset = got[:, :, width : width + chans] + got[:, :, width + chans : width + 2 * chans]
        square_total = jnp.sum(got[:, :, width + 2 * chans] + got[:, :, width + 2 * chans + 1], axis=0)
        inputs = lax.rsqrt(square_total / D + eps)[:, None] * total
        by_block = jnp.moveaxis(inputs.reshape(seqs, NZ, chans), 1, 0)
        own = lax.dynamic_index_in_dim(by_block, d_index, 0, keepdims=False)
        returned.append(turn(own))
        after = late[n]
        mix = joined(after[:, :, 2 * cols : 2 * cols + chans], after[:, :, 2 * cols + chans :])
        pre = offset + jnp.einsum("zrc,zco->zro", by_block, mix, precision=HIGHEST)
        mixed = jax.nn.gelu(pre).astype(jnp.bfloat16)
        mixed = jnp.moveaxis(mixed, 0, 1).reshape(seqs, width)
        out = jnp.dot(
            mixed,
            after[:, :, : 2 * cols].reshape(width, 2 * cols),
            preferred_element_type=jnp.float32,
        )
        if n < LAYERS - 1:
            sent = out.astype(jnp.bfloat16)
            for k in range(1, NY):
                out = out + shift_y(sent, k).astype(jnp.float32)
            value, gate = out[:, :cols], out[:, cols:]
            x = (x + value * jax.nn.sigmoid(gate)).astype(jnp.bfloat16).astype(jnp.float32)
        else:
            by_y = out.reshape(NY, rows, 2 * cols)
            total = lax.dynamic_index_in_dim(by_y, y_index, 0, keepdims=False)
            for k in range(1, NY):
                target = (y_index + k) % NY
                block = lax.dynamic_index_in_dim(by_y, target, 0, keepdims=False)
                total = total + shift_y(block.astype(jnp.bfloat16), k).astype(jnp.float32)
            value, gate = total[:, :cols], total[:, cols:]
            mine = lax.dynamic_index_in_dim(x.reshape(NY, rows, cols), y_index, 0, keepdims=False)
            x = (mine + value * jax.nn.sigmoid(gate)).astype(jnp.bfloat16)

    states = []
    for n in range(LAYERS):
        base, drive, _, _ = prepared[n]
        grouped = returned[n].reshape(base.shape[0], base.shape[1], -1)
        states.append(base + jnp.einsum("gpc,rgc->rgp", drive, grouped, precision=HIGHEST))
    return (x, jnp.stack(states))


def solution(mesh):
    grid = Mesh(mesh.devices.reshape(NZ, NY, NX, NC), ALL)
    return jax.shard_map(
        per_device,
        mesh=grid,
        in_specs=(
            P(TP, DP),
            P(None, DP),
            P(None, DP, TP),
            P(None, TP, None),
            P(None, TP, None),
            P(None, TP),
            P(None, TP, None, None),
            P(None, TP, None, None),
            P(None, TP, None, None),
            P(None, TP, None, None),
            P(None, TP),
            P(None, TP, DP),
            P(None, TP, DP),
            P(None, DP, TP, None),
        ),
        out_specs=(P(TP, DP), P(None, DP, TP, None)),
        check_vma=False,
    )
```

```python
import functools

import jax
import jax.numpy as jnp
from jax import lax
from jax.experimental import pallas as pl
from jax.experimental.pallas import tpu as pltpu
from jax.sharding import Mesh
from jax.sharding import PartitionSpec as P

D = 2048
LAYERS = 2
NZ, NY, NX, NC = 8, 4, 4, 2
ND = NX * NC
TP = ("z", "y")
DP = ("x", "c")
ALL = ("z", "y", "x", "c")
ROWS = 8
SEQS = NY * ROWS
COLS = 256
BLOCK = 64
WIDTH = NZ * BLOCK
PAY = 1024

eps = 1e-06
HIGHEST = lax.Precision.HIGHEST
f32 = jnp.float32
bf16 = jnp.bfloat16


def turn(value):
    pairs = []
    for z in range(NZ):
        for y in range(NY):
            for d in range(ND):
                pairs.append(((z * NY + y) * ND + d, (d * NY + y) * ND + z))
    return lax.ppermute(value, ALL, pairs)


def shift_y(value, k):
    return lax.ppermute(value, "y", [(i, (i + k) % NY) for i in range(NY)])


def shift_z(value, k):
    return lax.ppermute(value, "z", [(i, (i + k) % NZ) for i in range(NZ)])


def ring_z(own):
    up1 = shift_z(own, 1)
    down1 = shift_z(own, -1)
    up2 = shift_z(up1, 1)
    down2 = shift_z(down1, -1)
    up3 = shift_z(up2, 1)
    down3 = shift_z(down2, -1)
    up4 = shift_z(up3, 1)
    return [own, up1, up2, up3, up4, down3, down2, down1]


def two_halves(value):
    high = value.astype(bf16)
    low = (value - high.astype(f32)).astype(bf16)
    return high, low


def prepare(old_state, lam_re, lam_im, log_dt, b_re, b_im, readout_real, readout_imaginary, d_skip):
    half = old_state.shape[-1] // 2
    step_size = jnp.exp(log_dt)[:, None]
    decay = jnp.exp(lam_re * step_size)
    angle = lam_im * step_size
    keep_re = decay * jnp.cos(angle)
    keep_im = decay * jnp.sin(angle)
    denom = lam_re * lam_re + lam_im * lam_im
    ratio_re = ((keep_re - 1.0) * lam_re + keep_im * lam_im) / denom
    ratio_im = (keep_im * lam_re - (keep_re - 1.0) * lam_im) / denom
    drive_re = ratio_re[..., None] * b_re - ratio_im[..., None] * b_im
    drive_im = ratio_re[..., None] * b_im + ratio_im[..., None] * b_re
    drive = jnp.concatenate([drive_re, drive_im], axis=1)
    read = jnp.concatenate([readout_real, -readout_imaginary], axis=2)
    old_re = old_state[..., :half]
    old_im = old_state[..., half:]
    base = jnp.concatenate(
        [keep_re * old_re - keep_im * old_im, keep_re * old_im + keep_im * old_re], axis=-1
    )
    groups, chans = read.shape[:2]
    offset = jnp.einsum("rgp,gop->rgo", base, read, precision=HIGHEST)
    offset = offset.reshape(offset.shape[0], groups * chans)
    inner = jnp.einsum("gpc,gop->gco", drive, read, precision=HIGHEST)
    eye = jnp.eye(groups, dtype=f32)
    mix = (inner[:, :, None, :] * eye[:, None, :, None]).reshape(groups * chans, groups * chans)
    mix = mix + jnp.eye(groups * chans, dtype=f32) * d_skip[None, :]
    return base, drive, offset, mix


def side_payload(offset, mix):
    o_high, o_low = two_halves(offset)
    m_high, m_low = two_halves(mix)
    half = BLOCK // 2
    return jnp.concatenate(
        [
            o_high,
            o_low,
            jnp.zeros((SEQS, 128), bf16),
            m_high[:half],
            m_high[half:],
            m_low[:half],
            m_low[half:],
        ],
        axis=1,
    )


def write_payload(pay_ref, x, gain, side, blocks):
    squares = jnp.sum(x * x, axis=1, keepdims=True)
    s_high, s_low = two_halves(squares)
    lane = lax.broadcasted_iota(jnp.int32, (SEQS, 128), 1)
    s_part = jnp.where(lane == 0, s_high.astype(f32), jnp.where(lane == 1, s_low.astype(f32), 0.0))
    parts = [blocks[j] for j in range(NZ)]
    row = jnp.concatenate(parts, axis=1).astype(bf16)
    for i in range(ND):
        pay_ref[i, :, :WIDTH] = row
        pay_ref[i, :, WIDTH : WIDTH + 128] = side[:, :128]
        pay_ref[i, :, WIDTH + 128 : WIDTH + 256] = s_part.astype(bf16)
        pay_ref[i, :, WIDTH + 256 :] = side[:, 256:]


def times_turned(left, right):
    return lax.dot_general(left, right, (((1,), (1,)), ((), ())), preferred_element_type=f32)


def first_kernel(p0, p1, p2, p3, gain, side, w, pay_ref, x_ref, rows):
    y = lax.axis_index("y")
    for k, piece in enumerate((p0, p1, p2, p3)):
        rows[lax.rem(y + NY - k, NY)] = piece[...].astype(f32)
    x = rows[...].reshape(SEQS, COLS)
    x_ref[...] = x
    normed = (x * gain[...]).astype(bf16)
    blocks = [times_turned(normed, w[j]) for j in range(NZ)]
    write_payload(pay_ref, x, gain, side[...], blocks)


def next_kernel(out, r1, r2, r3, x_old, gain, side, *refs):
    w = refs[:NZ]
    pay_ref, x_ref, blocks = refs[NZ:]
    z = lax.axis_index("z")
    total = out[...] + r1[...] + r2[...] + r3[...]
    x = x_old[...] + total[:, :COLS] * jax.nn.sigmoid(total[:, COLS:])
    x = x.astype(bf16).astype(f32)
    x_ref[...] = x
    normed = (x * gain[...]).astype(bf16)
    for k in range(NZ):
        blocks[lax.rem(z + NZ - k, NZ)] = times_turned(normed, w[k][...])
    write_payload(pay_ref, x, gain, side[...], blocks)


def mid_kernel(last, got, *refs):
    w = refs[:NZ]
    rest = refs[NZ:]
    if last:
        own_out, s1, s2, s3, own_u, u_blocks, mixed, ordered, weights, by_y = rest
    else:
        own_out, own_u, u_blocks, mixed, ordered, weights = rest
    z = lax.axis_index("z")
    d = lax.axis_index("x") * NC + lax.axis_index("c")
    total = got[0, :, :WIDTH].astype(f32)
    squares = got[0, :, WIDTH + 128 : WIDTH + 256].astype(f32)
    for i in range(1, ND):
        total = total + got[i, :, :WIDTH].astype(f32)
        squares = squares + got[i, :, WIDTH + 128 : WIDTH + 256].astype(f32)
    factor = lax.rsqrt(jnp.sum(squares, axis=1, keepdims=True) / D + eps)
    u = total * factor
    half = BLOCK // 2
    for j in range(NZ):
        part = u[:, j * BLOCK : (j + 1) * BLOCK]
        u_blocks[j] = part
        offset = got[j, :, WIDTH : WIDTH + BLOCK].astype(f32) + got[
            j, :, WIDTH + BLOCK : WIDTH + 2 * BLOCK
        ].astype(f32)
        high, low = two_halves(part)
        m = got[j, :, WIDTH + 256 :]
        m_high = jnp.concatenate([m[:, :BLOCK], m[:, BLOCK : 2 * BLOCK]], axis=0)
        m_low = jnp.concatenate([m[:, 2 * BLOCK : 3 * BLOCK], m[:, 3 * BLOCK :]], axis=0)
        pre = (
            offset
            + jnp.dot(high, m_low, preferred_element_type=f32)
            + jnp.dot(low, m_high, preferred_element_type=f32)
            + jnp.dot(high, m_high, preferred_element_type=f32)
        )
        mixed[j] = jax.nn.gelu(pre)
    own_u[...] = u_blocks[d]
    for k in range(NZ):
        ordered[:, k * BLOCK : (k + 1) * BLOCK] = mixed[lax.rem(z + NZ - k, NZ)].astype(bf16)
        weights[k * BLOCK : (k + 1) * BLOCK, :] = w[k][...]
    out = jnp.dot(ordered[...], weights[...], preferred_element_type=f32)
    if last:
        y = lax.axis_index("y")
        by_y[...] = out.reshape(NY, ROWS, 2 * COLS)
        own_out[...] = by_y[y]
        for k, ref in enumerate((s1, s2, s3), 1):
            ref[...] = by_y[lax.rem(y + k, NY)]
    else:
        own_out[...] = out


def whole(*arrays):
    return [pl.BlockSpec(a.shape, functools.partial(lambda n, i: (0,) * n, a.ndim)) for a in arrays]


def call(body, args, windows, outs, scratch, flops):
    in_specs = whole(*args)
    for _, cols, index in windows:
        in_specs.append(pl.BlockSpec((BLOCK, cols), functools.partial(lambda n, i: (0, n), index)))
    return pl.pallas_call(
        body,
        grid=(1,),
        in_specs=in_specs,
        out_specs=whole(*outs),
        out_shape=outs,
        scratch_shapes=scratch,
        cost_estimate=pl.CostEstimate(flops=flops, bytes_accessed=1 << 20, transcendentals=0),
    )(*args, *[a for a, _, _ in windows])


def shape(dims, dtype):
    return jax.ShapeDtypeStruct(dims, dtype)


PAY_OUTS = [shape((ND, SEQS, PAY), bf16), shape((SEQS, COLS), f32)]
MID_SCRATCH = [
    pltpu.VMEM((NZ, SEQS, BLOCK), f32),
    pltpu.VMEM((NZ, SEQS, BLOCK), f32),
    pltpu.VMEM((SEQS, WIDTH), bf16),
    pltpu.VMEM((WIDTH, 2 * COLS), bf16),
]


def per_device(
    stream,
    norm_gain,
    w_input,
    lam_re,
    lam_im,
    log_dt,
    b_re,
    b_im,
    readout_real,
    readout_imaginary,
    d_skip,
    w_val,
    w_gate,
    state,
):
    y_index = lax.axis_index("y")
    pieces = [stream] + [shift_y(stream, k) for k in range(1, NY)]
    late = jnp.concatenate([w_val[0], w_gate[0], w_val[1], w_gate[1], w_input[1].T], axis=1)
    ring = ring_z(late)
    first_w = lax.all_to_all(
        jnp.broadcast_to(w_input[0].T[None], (NZ, BLOCK, COLS)), "z", 0, 0, tiled=True
    )

    prepared = [
        prepare(
            state[n],
            lam_re[n],
            lam_im[n],
            log_dt[n],
            b_re[n],
            b_im[n],
            readout_real[n],
            readout_imaginary[n],
            d_skip[n],
        )
        for n in range(LAYERS)
    ]
    carried = turn(jnp.stack([jnp.concatenate([p[2], p[3]]) for p in prepared]))
    sides = [side_payload(carried[n, :SEQS], carried[n, SEQS:]) for n in range(LAYERS)]

    payload, x = call(
        first_kernel,
        [*pieces, norm_gain[0:1], sides[0], first_w],
        [],
        PAY_OUTS,
        [pltpu.VMEM((NY, ROWS, COLS), f32)],
        1 << 24,
    )
    got = lax.all_to_all(payload, DP, 0, 0, tiled=True)
    out, u0 = call(
        functools.partial(mid_kernel, False),
        [got],
        [(w, 2 * COLS, 0) for w in ring],
        [shape((SEQS, 2 * COLS), f32), shape((SEQS, BLOCK), f32)],
        MID_SCRATCH,
        1 << 24,
    )
    others = [shift_y(out, k) for k in range(1, NY)]
    payload, x = call(
        next_kernel,
        [out, *others, x, norm_gain[1:2], sides[1]],
        [(w, COLS, 4) for w in ring],
        PAY_OUTS,
        [pltpu.VMEM((NZ, SEQS, BLOCK), f32)],
        1 << 24,
    )
    got = lax.all_to_all(payload, DP, 0, 0, tiled=True)
    block = shape((ROWS, 2 * COLS), f32)
    own, s1, s2, s3, u1 = call(
        functools.partial(mid_kernel, True),
        [got],
        [(w, 2 * COLS, 1) for w in ring],
        [block, block, block, block, shape((SEQS, BLOCK), f32)],
        MID_SCRATCH + [pltpu.VMEM((NY, ROWS, 2 * COLS), f32)],
        1 << 24,
    )
    returned = [turn(u0), turn(u1)]
    for k, sent in enumerate((s1, s2, s3), 1):
        own = own + shift_y(sent, k)
    mine = lax.dynamic_index_in_dim(x.reshape(NY, ROWS, COLS), y_index, 0, keepdims=False)
    stream = (mine + own[:, :COLS] * jax.nn.sigmoid(own[:, COLS:])).astype(bf16)

    states = []
    for n in range(LAYERS):
        base, drive, _, _ = prepared[n]
        grouped = returned[n].reshape(base.shape[0], base.shape[1], -1)
        states.append(base + jnp.einsum("gpc,rgc->rgp", drive, grouped, precision=HIGHEST))
    return (stream, jnp.stack(states))


def solution(mesh):
    grid = Mesh(mesh.devices.reshape(NZ, NY, NX, NC), ALL)
    return jax.shard_map(
        per_device,
        mesh=grid,
        in_specs=(
            P(TP, DP),
            P(None, DP),
            P(None, DP, TP),
            P(None, TP, None),
            P(None, TP, None),
            P(None, TP),
            P(None, TP, None, None),
            P(None, TP, None, None),
            P(None, TP, None, None),
            P(None, TP, None, None),
            P(None, TP),
            P(None, TP, DP),
            P(None, TP, DP),
            P(None, DP, TP, None),
        ),
        out_specs=(P(TP, DP), P(None, DP, TP, None)),
        check_vma=False,
    )
```

```python
import jax
import jax.numpy as jnp
from jax import lax
from jax.experimental import pallas as pl
from jax.experimental.pallas import tpu as pltpu
from jax.sharding import Mesh
from jax.sharding import PartitionSpec as P

D = 2048
LAYERS = 2
NZ, NY, NX, NC = 8, 4, 4, 2
ND = NX * NC
TP = ("z", "y")
DP = ("x", "c")
ALL = ("z", "y", "x", "c")
ROWS = 8
SEQS = NY * ROWS
COLS = 256
BLOCK = 64
WIDTH = NZ * BLOCK
PAY = 1024

eps = 1e-06
HIGHEST = lax.Precision.HIGHEST
f32 = jnp.float32
bf16 = jnp.bfloat16


def turn(value):
    pairs = []
    for z in range(NZ):
        for y in range(NY):
            for d in range(ND):
                pairs.append(((z * NY + y) * ND + d, (d * NY + y) * ND + z))
    return lax.ppermute(value, ALL, pairs)


def shift_y(value, k):
    return lax.ppermute(value, "y", [(i, (i + k) % NY) for i in range(NY)])


def shift_z(value, k):
    return lax.ppermute(value, "z", [(i, (i + k) % NZ) for i in range(NZ)])


def ring_z(own):
    up1 = shift_z(own, 1)
    down1 = shift_z(own, -1)
    up2 = shift_z(up1, 1)
    down2 = shift_z(down1, -1)
    up3 = shift_z(up2, 1)
    down3 = shift_z(down2, -1)
    up4 = shift_z(up3, 1)
    return [own, up1, up2, up3, up4, down3, down2, down1]


def two_halves(value):
    high = value.astype(bf16)
    low = (value - high.astype(f32)).astype(bf16)
    return high, low


def prep_kernel(lam_re, lam_im, log_dt, b_re, b_im, r_re, r_im, d_skip, state, base, drive, carried):
    groups, chans, half = b_re.shape[1:]
    size = groups * chans
    row = lax.broadcasted_iota(jnp.int32, (size, size), 0)
    col = lax.broadcasted_iota(jnp.int32, (size, size), 1)
    for n in range(LAYERS):
        steps = jnp.concatenate([jnp.full((1, half), log_dt[n, g], f32) for g in range(groups)])
        step = jnp.exp(steps)
        re, im = lam_re[n], lam_im[n]
        decay = jnp.exp(re * step)
        angle = im * step
        keep_re = decay * jnp.cos(angle)
        keep_im = decay * jnp.sin(angle)
        denom = re * re + im * im
        ratio_re = ((keep_re - 1.0) * re + keep_im * im) / denom
        ratio_im = (keep_im * re - (keep_re - 1.0) * im) / denom
        drives, reads, offsets = [], [], []
        for g in range(groups):
            q_re, q_im = ratio_re[g : g + 1], ratio_im[g : g + 1]
            d_re = q_re * b_re[n, g] - q_im * b_im[n, g]
            d_im = q_re * b_im[n, g] + q_im * b_re[n, g]
            drives.append(jnp.concatenate([d_re, d_im], axis=1))
            reads.append(jnp.concatenate([r_re[n, g], -r_im[n, g]], axis=1))
            k_re, k_im = keep_re[g : g + 1], keep_im[g : g + 1]
            old = state[n, :, g, :]
            swapped = jnp.concatenate([old[:, half:], old[:, :half]], axis=1)
            new = (
                jnp.concatenate([k_re, k_re], axis=1) * old
                + jnp.concatenate([-k_im, k_im], axis=1) * swapped
            )
            base[n, :, g, :] = new
            offsets.append(times_turned(new, reads[g], HIGHEST))
        dcat = jnp.concatenate(drives)
        drive[n] = dcat
        full = times_turned(dcat, jnp.concatenate(reads), HIGHEST)
        mix = jnp.where(row // chans == col // chans, full, 0.0)
        mix = mix + jnp.where(row == col, d_skip[n : n + 1, :], 0.0)
        carried[n, :SEQS, :] = jnp.concatenate(offsets, axis=1)
        carried[n, SEQS:, :] = mix


def write_payload(pay_ref, x, carried, blocks):
    squares = jnp.sum(x * x, axis=1, keepdims=True)
    s_high, s_low = two_halves(squares)
    lane = lax.broadcasted_iota(jnp.int32, (SEQS, 128), 1)
    s_part = jnp.where(lane == 0, s_high.astype(f32), jnp.where(lane == 1, s_low.astype(f32), 0.0))
    o_high, o_low = two_halves(carried[:SEQS])
    m_high, m_low = two_halves(carried[SEQS:])
    half = BLOCK // 2
    row = jnp.concatenate(
        [blocks[j].astype(bf16) for j in range(NZ)]
        + [o_high, o_low, s_part.astype(bf16), m_high[:half], m_high[half:], m_low[:half], m_low[half:]],
        axis=1,
    )
    for i in range(ND):
        pay_ref[i] = row


def times_turned(left, right, precision=None):
    return lax.dot_general(
        left, right, (((1,), (1,)), ((), ())), precision=precision, preferred_element_type=f32
    )


def first_kernel(p0, p1, p2, p3, gain, carried, w, pay_ref, x_ref, rows):
    y = lax.axis_index("y")
    for k, piece in enumerate((p0, p1, p2, p3)):
        rows[lax.rem(y + NY - k, NY)] = piece[...].astype(f32)
    x = rows[...].reshape(SEQS, COLS)
    x_ref[...] = x
    normed = (x * gain[0:1]).astype(bf16)
    blocks = [times_turned(normed, w[j]) for j in range(NZ)]
    write_payload(pay_ref, x, carried[0], blocks)


def next_kernel(out, r1, r2, r3, x_old, gain, carried, *refs):
    w = refs[:NZ]
    pay_ref, x_ref, blocks = refs[NZ:]
    z = lax.axis_index("z")
    total = out[...] + r1[...] + r2[...] + r3[...]
    x = x_old[...] + total[:, :COLS] * jax.nn.sigmoid(total[:, COLS:])
    x = x.astype(bf16).astype(f32)
    x_ref[...] = x
    normed = (x * gain[1:2]).astype(bf16)
    for k in range(NZ):
        blocks[lax.rem(z + NZ - k, NZ)] = times_turned(normed, w[k][:, 4 * COLS :])
    write_payload(pay_ref, x, carried[1], blocks)


def inputs_of(got):
    total = got[0, :, :WIDTH].astype(f32)
    squares = got[0, :, WIDTH + 128 : WIDTH + 256].astype(f32)
    for i in range(1, ND):
        total = total + got[i, :, :WIDTH].astype(f32)
        squares = squares + got[i, :, WIDTH + 128 : WIDTH + 256].astype(f32)
    return total * lax.rsqrt(jnp.sum(squares, axis=1, keepdims=True) / D + eps)


def gated(got, u, w, first_col, mixed, ordered, weights):
    z = lax.axis_index("z")
    for j in range(NZ):
        offset = got[j, :, WIDTH : WIDTH + BLOCK].astype(f32) + got[
            j, :, WIDTH + BLOCK : WIDTH + 2 * BLOCK
        ].astype(f32)
        high, low = two_halves(u[:, j * BLOCK : (j + 1) * BLOCK])
        m = got[j, :, WIDTH + 256 :]
        m_high = jnp.concatenate([m[:, :BLOCK], m[:, BLOCK : 2 * BLOCK]], axis=0)
        m_low = jnp.concatenate([m[:, 2 * BLOCK : 3 * BLOCK], m[:, 3 * BLOCK :]], axis=0)
        pre = (
            offset
            + jnp.dot(high, m_low, preferred_element_type=f32)
            + jnp.dot(low, m_high, preferred_element_type=f32)
            + jnp.dot(high, m_high, preferred_element_type=f32)
        )
        mixed[j] = jax.nn.gelu(pre)
    for k in range(NZ):
        ordered[:, k * BLOCK : (k + 1) * BLOCK] = mixed[lax.rem(z + NZ - k, NZ)].astype(bf16)
        weights[k * BLOCK : (k + 1) * BLOCK, :] = w[k][:, first_col : first_col + 2 * COLS]
    return jnp.dot(ordered[...], weights[...], preferred_element_type=f32)


def own_block(u, u_blocks):
    d = lax.axis_index("x") * NC + lax.axis_index("c")
    for j in range(NZ):
        u_blocks[j] = u[:, j * BLOCK : (j + 1) * BLOCK]
    return u_blocks[d]


def mid_kernel(got, *refs):
    w = refs[:NZ]
    out, own_u, u_blocks, mixed, ordered, weights = refs[NZ:]
    u = inputs_of(got)
    own_u[...] = own_block(u, u_blocks)
    out[...] = gated(got, u, w, 0, mixed, ordered, weights)


def inputs_kernel(got, u_ref, own_u, u_blocks):
    u = inputs_of(got)
    u_ref[...] = u
    own_u[...] = own_block(u, u_blocks)


def last_kernel(got, u, *refs):
    w = refs[:NZ]
    own_out, s1, s2, s3, mixed, ordered, weights, by_y = refs[NZ:]
    out = gated(got, u[...], w, 2 * COLS, mixed, ordered, weights)
    y = lax.axis_index("y")
    by_y[...] = out.reshape(NY, ROWS, 2 * COLS)
    own_out[...] = by_y[y]
    for k, ref in enumerate((s1, s2, s3), 1):
        ref[...] = by_y[lax.rem(y + k, NY)]


def stream_kernel(own, r1, r2, r3, x, out):
    y = lax.axis_index("y")
    total = own[...] + r1[...] + r2[...] + r3[...]
    mine = x[pl.ds(pl.multiple_of(y * ROWS, ROWS), ROWS), :]
    out[...] = (mine + total[:, :COLS] * jax.nn.sigmoid(total[:, COLS:])).astype(bf16)


def states_kernel(base, drive, u0, u1, out):
    groups = base.shape[2]
    chans = BLOCK // groups
    for n, u in enumerate((u0, u1)):
        for g in range(groups):
            cut = slice(g * chans, (g + 1) * chans)
            push = jnp.dot(u[:, cut], drive[n, cut, :], precision=HIGHEST, preferred_element_type=f32)
            out[n, :, g, :] = base[n, :, g, :] + push


def call(body, args, outs, scratch=(), scalar=None):
    spaces = [pltpu.SMEM if i == scalar else pltpu.VMEM for i in range(len(args))]
    return pl.pallas_call(
        body,
        in_specs=[pl.BlockSpec(memory_space=s) for s in spaces],
        out_specs=[pl.BlockSpec(memory_space=pltpu.VMEM) for _ in outs],
        out_shape=outs,
        scratch_shapes=list(scratch),
        compiler_params=pltpu.CompilerParams(vmem_limit_bytes=12 << 20),
        cost_estimate=pl.CostEstimate(flops=1 << 24, bytes_accessed=1 << 20, transcendentals=0),
    )(*args)


def shape(dims, dtype=f32):
    return jax.ShapeDtypeStruct(dims, dtype)


PAY_OUTS = [shape((ND, SEQS, PAY), bf16), shape((SEQS, COLS))]
BLOCKS = pltpu.VMEM((NZ, SEQS, BLOCK), f32)
GATED = [BLOCKS, pltpu.VMEM((SEQS, WIDTH), bf16), pltpu.VMEM((WIDTH, 2 * COLS), bf16)]


def both_layers(
    stream,
    norm_gain,
    w_input,
    lam_re,
    lam_im,
    log_dt,
    b_re,
    b_im,
    readout_real,
    readout_imaginary,
    d_skip,
    w_val,
    w_gate,
    state,
):
    w_turned = jnp.swapaxes(w_input, 1, 2)
    first_w = lax.all_to_all(
        jnp.broadcast_to(w_turned[0][None], (NZ, BLOCK, COLS)), "z", 0, 0, tiled=True
    )
    pieces = [stream] + [shift_y(stream, k) for k in range(1, NY)]
    late = jnp.concatenate([w_val[0], w_gate[0], w_val[1], w_gate[1], w_turned[1]], axis=1)
    ring = ring_z(late)

    base, drive, own = call(
        prep_kernel,
        [
            lam_re,
            lam_im,
            log_dt,
            jnp.swapaxes(b_re, 2, 3),
            jnp.swapaxes(b_im, 2, 3),
            readout_real,
            readout_imaginary,
            d_skip,
            state,
        ],
        [
            shape(state.shape),
            shape((LAYERS, BLOCK, state.shape[-1])),
            shape((LAYERS, SEQS + BLOCK, BLOCK)),
        ],
        scalar=2,
    )
    carried = turn(own)

    payload, x = call(
        first_kernel,
        [*pieces, norm_gain, carried, first_w],
        PAY_OUTS,
        [pltpu.VMEM((NY, ROWS, COLS), f32)],
    )
    got = lax.all_to_all(payload, DP, 0, 0, tiled=True)
    out, u0 = call(
        mid_kernel,
        [got, *ring],
        [shape((SEQS, 2 * COLS)), shape((SEQS, BLOCK))],
        [BLOCKS, *GATED],
    )
    others = [shift_y(out, k) for k in range(1, NY)]
    u0 = turn(u0)
    payload, x = call(next_kernel, [out, *others, x, norm_gain, carried, *ring], PAY_OUTS, [BLOCKS])
    got = lax.all_to_all(payload, DP, 0, 0, tiled=True)
    u, u1 = call(
        inputs_kernel, [got], [shape((SEQS, WIDTH)), shape((SEQS, BLOCK))], [BLOCKS]
    )
    u1 = turn(u1)
    own, s1, s2, s3 = call(
        last_kernel,
        [got, u, *ring],
        [shape((ROWS, 2 * COLS))] * NY,
        [*GATED, pltpu.VMEM((NY, ROWS, 2 * COLS), f32)],
    )
    others = [shift_y(sent, k) for k, sent in enumerate((s1, s2, s3), 1)]
    (stream,) = call(stream_kernel, [own, *others, x], [shape((ROWS, COLS), bf16)])
    (states,) = call(states_kernel, [base, drive, u0, u1], [shape(state.shape)])
    return (stream, states)


def solution(mesh):
    grid = Mesh(mesh.devices.reshape(NZ, NY, NX, NC), ALL)
    return jax.shard_map(
        both_layers,
        mesh=grid,
        in_specs=(
            P(TP, DP),
            P(None, DP),
            P(None, DP, TP),
            P(None, TP, None),
            P(None, TP, None),
            P(None, TP),
            P(None, TP, None, None),
            P(None, TP, None, None),
            P(None, TP, None, None),
            P(None, TP, None, None),
            P(None, TP),
            P(None, TP, DP),
            P(None, TP, DP),
            P(None, DP, TP, None),
        ),
        out_specs=(P(TP, DP), P(None, DP, TP, None)),
        check_vma=False,
    )
```

```python
import jax
import jax.numpy as jnp
from jax import lax
from jax.experimental import pallas as pl
from jax.experimental.pallas import tpu as pltpu
from jax.sharding import Mesh
from jax.sharding import PartitionSpec as P

D = 2048
LAYERS = 2
NZ, NY, NX, NC = 8, 4, 4, 2
ND = NX * NC
TP = ("z", "y")
DP = ("x", "c")
ALL = ("z", "y", "x", "c")
ROWS = 8
SEQS = NY * ROWS
COLS = 256
BLOCK = 64
WIDTH = NZ * BLOCK

eps = 1e-06
HIGHEST = lax.Precision.HIGHEST
f32 = jnp.float32
bf16 = jnp.bfloat16


STEP_X = (2, 3, 1, 0, 0, 1, 3, 2)
STEP_C = (1, 1, 1, 1, 0, 0, 0, 0)


def place(z, delta):
    return lax.rem(lax.div(z, 2) + STEP_X[delta], NX) * NC + STEP_C[delta]


def turn(value, back=False):
    pairs = []
    for z in range(NZ):
        for y in range(NY):
            for delta in range(NZ):
                owner = ((z + delta) % NZ * NY + y) * ND + z
                d = (z // 2 + STEP_X[delta]) % NX * NC + STEP_C[delta]
                user = (z * NY + y) * ND + d
                pairs.append((user, owner) if back else (owner, user))
    return lax.ppermute(value, ALL, pairs)


def shift_y(value, k):
    return lax.ppermute(value, "y", [(i, (i + k) % NY) for i in range(NY)])


def shift_z(value, k):
    return lax.ppermute(value, "z", [(i, (i + k) % NZ) for i in range(NZ)])


def ring_z(own):
    up1 = shift_z(own, 1)
    down1 = shift_z(own, -1)
    up2 = shift_z(up1, 1)
    down2 = shift_z(down1, -1)
    up3 = shift_z(up2, 1)
    down3 = shift_z(down2, -1)
    up4 = shift_z(up3, 1)
    return [own, up1, up2, up3, up4, down3, down2, down1]


def two_halves(value):
    high = value.astype(bf16)
    low = (value - high.astype(f32)).astype(bf16)
    return high, low


def pack_kernel(w_in, w_val, w_gate, out):
    row = jnp.concatenate([w_in[0], w_val[0], w_gate[0]], axis=1)
    for i in range(NZ):
        out[i] = row


def prep_kernel(
    lam_re,
    lam_im,
    log_dt,
    b_re,
    b_im,
    r_re,
    r_im,
    d_skip,
    state,
    w_in,
    w_val,
    w_gate,
    base,
    drive,
    carried,
    late,
):
    groups, chans, half = b_re.shape[1:]
    size = groups * chans
    row = lax.broadcasted_iota(jnp.int32, (size, size), 0)
    col = lax.broadcasted_iota(jnp.int32, (size, size), 1)
    for n in range(LAYERS):
        steps = jnp.concatenate([jnp.full((1, half), log_dt[n, g], f32) for g in range(groups)])
        step = jnp.exp(steps)
        re, im = lam_re[n], lam_im[n]
        decay = jnp.exp(re * step)
        angle = im * step
        keep_re = decay * jnp.cos(angle)
        keep_im = decay * jnp.sin(angle)
        denom = re * re + im * im
        ratio_re = ((keep_re - 1.0) * re + keep_im * im) / denom
        ratio_im = (keep_im * re - (keep_re - 1.0) * im) / denom
        drives, reads, offsets = [], [], []
        for g in range(groups):
            q_re, q_im = ratio_re[g : g + 1], ratio_im[g : g + 1]
            d_re = q_re * b_re[n, g] - q_im * b_im[n, g]
            d_im = q_re * b_im[n, g] + q_im * b_re[n, g]
            drives.append(jnp.concatenate([d_re, d_im], axis=1))
            reads.append(jnp.concatenate([r_re[n, g], -r_im[n, g]], axis=1))
            k_re, k_im = keep_re[g : g + 1], keep_im[g : g + 1]
            old = state[n, :, g, :]
            swapped = jnp.concatenate([old[:, half:], old[:, :half]], axis=1)
            new = (
                jnp.concatenate([k_re, k_re], axis=1) * old
                + jnp.concatenate([-k_im, k_im], axis=1) * swapped
            )
            base[n, :, g, :] = new
            offsets.append(times_turned(new, reads[g], HIGHEST))
        dcat = jnp.concatenate(drives)
        drive[n] = dcat
        full = times_turned(dcat, jnp.concatenate(reads), HIGHEST)
        mix = jnp.where(row // chans == col // chans, full, 0.0)
        mix = mix + jnp.where(row == col, d_skip[n : n + 1, :], 0.0)
        carried[n * SEQS : (n + 1) * SEQS, :] = jnp.concatenate(offsets, axis=1)
        if n == 0:
            carried[LAYERS * SEQS :, :] = mix
        else:
            late[...] = jnp.concatenate([w_val[n], w_gate[n], w_in[n], *two_halves(mix)], axis=1)


def write_payload(pay_ref, x, blocks, offset, mix=None):
    squares = jnp.sum(x * x, axis=1, keepdims=True)
    s_high, s_low = two_halves(squares)
    lane = lax.broadcasted_iota(jnp.int32, (SEQS, 128), 1)
    s_part = jnp.where(lane == 0, s_high.astype(f32), jnp.where(lane == 1, s_low.astype(f32), 0.0))
    parts = [blocks[j].astype(bf16) for j in range(NZ)]
    parts += [*two_halves(offset), s_part.astype(bf16)]
    if mix is not None:
        half = BLOCK // 2
        for m in two_halves(mix):
            parts += [m[:half], m[half:]]
    row = jnp.concatenate(parts, axis=1)
    for i in range(ND):
        pay_ref[i] = row


def times_turned(left, right, precision=None):
    return lax.dot_general(
        left, right, (((1,), (1,)), ((), ())), precision=precision, preferred_element_type=f32
    )


def first_kernel(p0, p1, p2, p3, gain, carried, w, up, down, pay_ref, x_ref, rows):
    y = lax.axis_index("y")
    for k, piece in enumerate((p0, p1, p2, p3)):
        rows[lax.rem(y + NY - k, NY)] = piece[...].astype(f32)
    x = rows[...].reshape(SEQS, COLS)
    x_ref[...] = x
    normed = (x * gain[0:1]).astype(bf16)
    blocks = [times_turned(normed, w[j, :, :COLS]) for j in range(NZ)]
    write_payload(pay_ref, x, blocks, carried[:SEQS], carried[LAYERS * SEQS :])


def next_kernel(out, r1, r2, r3, x_old, gain, carried, *refs):
    w = refs[:NZ]
    pay_ref, x_ref, blocks = refs[NZ:]
    z = lax.axis_index("z")
    total = out[...] + r1[...] + r2[...] + r3[...]
    x = x_old[...] + total[:, :COLS] * jax.nn.sigmoid(total[:, COLS:])
    x = x.astype(bf16).astype(f32)
    x_ref[...] = x
    normed = (x * gain[1:2]).astype(bf16)
    for k in range(NZ):
        blocks[lax.rem(z + NZ - k, NZ)] = times_turned(normed, w[k][:, 2 * COLS : 3 * COLS])
    write_payload(pay_ref, x, blocks, carried[SEQS : LAYERS * SEQS])


def inputs_of(got):
    total = got[0, :, :WIDTH].astype(f32)
    squares = got[0, :, WIDTH + 128 : WIDTH + 256].astype(f32)
    for i in range(1, ND):
        total = total + got[i, :, :WIDTH].astype(f32)
        squares = squares + got[i, :, WIDTH + 128 : WIDTH + 256].astype(f32)
    return total * lax.rsqrt(jnp.sum(squares, axis=1, keepdims=True) / D + eps)


def gated(got, u_blocks, w, ordered, weights):
    z = lax.axis_index("z")
    for delta in range(NZ):
        block, slot, source = lax.rem(z + delta, NZ), (NZ - delta) % NZ, place(z, delta)
        sent = got[source]
        offset = sent[:, WIDTH : WIDTH + BLOCK].astype(f32)
        offset = offset + sent[:, WIDTH + BLOCK : WIDTH + 2 * BLOCK].astype(f32)
        cut = slice(slot * BLOCK, (slot + 1) * BLOCK)
        if isinstance(w, list):
            m_high = w[slot][:, 3 * COLS : 3 * COLS + BLOCK]
            m_low = w[slot][:, 3 * COLS + BLOCK :]
            weights[cut, :] = w[slot][:, : 2 * COLS]
        else:
            m = sent[:, WIDTH + 256 :]
            m_high = jnp.concatenate([m[:, :BLOCK], m[:, BLOCK : 2 * BLOCK]], axis=0)
            m_low = jnp.concatenate([m[:, 2 * BLOCK : 3 * BLOCK], m[:, 3 * BLOCK :]], axis=0)
            weights[cut, :] = w[block][:, COLS:]
        high, low = two_halves(u_blocks[block])
        pre = (
            offset
            + jnp.dot(high, m_low, preferred_element_type=f32)
            + jnp.dot(low, m_high, preferred_element_type=f32)
            + jnp.dot(high, m_high, preferred_element_type=f32)
        )
        ordered[:, cut] = jax.nn.gelu(pre).astype(bf16)
    return jnp.dot(ordered[...], weights[...], preferred_element_type=f32)


def own_block(u_blocks):
    z = lax.axis_index("z")
    d = lax.axis_index("x") * NC + lax.axis_index("c")
    delta = jnp.int32(0)
    for other in range(1, NZ):
        delta = jnp.where(place(z, other) == d, other, delta)
    return u_blocks[lax.rem(z + delta, NZ)]


def split_blocks(u, u_blocks):
    for j in range(NZ):
        u_blocks[j] = u[:, j * BLOCK : (j + 1) * BLOCK]


def mid_kernel(got, w, out, own_u, u_blocks, ordered, weights):
    split_blocks(inputs_of(got), u_blocks)
    own_u[...] = own_block(u_blocks)
    out[...] = gated(got, u_blocks, w, ordered, weights)


def inputs_kernel(got, earlier, u_blocks, own_u):
    split_blocks(inputs_of(got), u_blocks)
    own_u[...] = own_block(u_blocks)


def last_kernel(got, u_blocks, *refs):
    w = list(refs[:NZ])
    own_out, s1, s2, s3, ordered, weights, by_y = refs[NZ:]
    out = gated(got, u_blocks, w, ordered, weights)
    y = lax.axis_index("y")
    by_y[...] = out.reshape(NY, ROWS, 2 * COLS)
    own_out[...] = by_y[y]
    for k, ref in enumerate((s1, s2, s3), 1):
        ref[...] = by_y[lax.rem(y + k, NY)]


def stream_kernel(own, r1, r2, r3, x, out):
    y = lax.axis_index("y")
    total = own[...] + r1[...] + r2[...] + r3[...]
    mine = x[pl.ds(pl.multiple_of(y * ROWS, ROWS), ROWS), :]
    out[...] = (mine + total[:, :COLS] * jax.nn.sigmoid(total[:, COLS:])).astype(bf16)


def states_kernel(base, drive, u0, u1, out):
    groups = base.shape[2]
    chans = BLOCK // groups
    for n, u in enumerate((u0, u1)):
        for g in range(groups):
            cut = slice(g * chans, (g + 1) * chans)
            push = jnp.dot(u[:, cut], drive[n, cut, :], precision=HIGHEST, preferred_element_type=f32)
            out[n, :, g, :] = base[n, :, g, :] + push


def call(body, args, outs, scratch=(), scalar=None):
    spaces = [pltpu.SMEM if i == scalar else pltpu.VMEM for i in range(len(args))]
    return pl.pallas_call(
        body,
        in_specs=[pl.BlockSpec(memory_space=s) for s in spaces],
        out_specs=[pl.BlockSpec(memory_space=pltpu.VMEM) for _ in outs],
        out_shape=outs,
        scratch_shapes=list(scratch),
        compiler_params=pltpu.CompilerParams(vmem_limit_bytes=12 << 20),
        cost_estimate=pl.CostEstimate(flops=1 << 24, bytes_accessed=1 << 20, transcendentals=0),
    )(*args)


def shape(dims, dtype=f32):
    return jax.ShapeDtypeStruct(dims, dtype)


FIRST_PAY = WIDTH + 512
NEXT_PAY = WIDTH + 256
BLOCKS = pltpu.VMEM((NZ, SEQS, BLOCK), f32)
GATED = [pltpu.VMEM((SEQS, WIDTH), bf16), pltpu.VMEM((WIDTH, 2 * COLS), bf16)]


def both_layers(
    stream,
    norm_gain,
    w_input,
    lam_re,
    lam_im,
    log_dt,
    b_re,
    b_im,
    readout_real,
    readout_imaginary,
    d_skip,
    w_val,
    w_gate,
    state,
):
    w_turned = jnp.swapaxes(w_input, 1, 2)
    (packed,) = call(pack_kernel, [w_turned, w_val, w_gate], [shape((NZ, BLOCK, 3 * COLS), bf16)])
    first_w = lax.all_to_all(packed, "z", 0, 0, tiled=True)
    pieces = [stream] + [shift_y(stream, k) for k in range(1, NY)]
    base, drive, own, late = call(
        prep_kernel,
        [
            lam_re,
            lam_im,
            log_dt,
            jnp.swapaxes(b_re, 2, 3),
            jnp.swapaxes(b_im, 2, 3),
            readout_real,
            readout_imaginary,
            d_skip,
            state,
            w_turned,
            w_val,
            w_gate,
        ],
        [
            shape(state.shape),
            shape((LAYERS, BLOCK, state.shape[-1])),
            shape((LAYERS * SEQS + BLOCK, BLOCK)),
            shape((BLOCK, 3 * COLS + 2 * BLOCK), bf16),
        ],
        scalar=2,
    )
    carried = turn(own)
    ring = ring_z(late)

    payload, x = call(
        first_kernel,
        [*pieces, norm_gain, carried, first_w, ring[1], ring[-1]],
        [shape((ND, SEQS, FIRST_PAY), bf16), shape((SEQS, COLS))],
        [pltpu.VMEM((NY, ROWS, COLS), f32)],
    )
    got = lax.all_to_all(payload, DP, 0, 0, tiled=True)
    out, u0 = call(
        mid_kernel,
        [got, first_w],
        [shape((SEQS, 2 * COLS)), shape((SEQS, BLOCK))],
        [BLOCKS, *GATED],
    )
    others = [shift_y(out, k) for k in range(1, NY)]
    u0 = turn(u0, back=True)
    payload, x = call(
        next_kernel,
        [out, *others, x, norm_gain, carried, *ring],
        [shape((ND, SEQS, NEXT_PAY), bf16), shape((SEQS, COLS))],
        [BLOCKS],
    )
    got = lax.all_to_all(payload, DP, 0, 0, tiled=True)
    u, u1 = call(
        inputs_kernel, [got, u0], [shape((NZ, SEQS, BLOCK)), shape((SEQS, BLOCK))]
    )
    u1 = turn(u1, back=True)
    own, s1, s2, s3 = call(
        last_kernel,
        [got, u, *ring],
        [shape((ROWS, 2 * COLS))] * NY,
        [*GATED, pltpu.VMEM((NY, ROWS, 2 * COLS), f32)],
    )
    others = [shift_y(sent, k) for k, sent in enumerate((s1, s2, s3), 1)]
    (stream,) = call(stream_kernel, [own, *others, x], [shape((ROWS, COLS), bf16)])
    (states,) = call(states_kernel, [base, drive, u0, u1], [shape(state.shape)])
    return (stream, states)


def solution(mesh):
    grid = Mesh(mesh.devices.reshape(NZ, NY, NX, NC), ALL)
    return jax.shard_map(
        both_layers,
        mesh=grid,
        in_specs=(
            P(TP, DP),
            P(None, DP),
            P(None, DP, TP),
            P(None, TP, None),
            P(None, TP, None),
            P(None, TP),
            P(None, TP, None, None),
            P(None, TP, None, None),
            P(None, TP, None, None),
            P(None, TP, None, None),
            P(None, TP),
            P(None, TP, DP),
            P(None, TP, DP),
            P(None, DP, TP, None),
        ),
        out_specs=(P(TP, DP), P(None, DP, TP, None)),
        check_vma=False,
    )
```

```python
import jax
import jax.numpy as jnp
from jax import lax
from jax.experimental import pallas as pl
from jax.experimental.pallas import tpu as pltpu
from jax.sharding import Mesh
from jax.sharding import PartitionSpec as P

D = 2048
LAYERS = 2
NZ, NY, NX, NC = 8, 4, 4, 2
ND = NX * NC
TP = ("z", "y")
DP = ("x", "c")
ALL = ("z", "y", "x", "c")
ROWS = 8
SEQS = NY * ROWS
COLS = 256
BLOCK = 64
WIDTH = NZ * BLOCK

eps = 1e-06
HIGHEST = lax.Precision.HIGHEST
f32 = jnp.float32
bf16 = jnp.bfloat16


STEP_X = (2, 3, 1, 0, 0, 1, 3, 2)
STEP_C = (1, 1, 1, 1, 0, 0, 0, 0)


def place(z, delta):
    return lax.rem(lax.div(z, 2) + STEP_X[delta], NX) * NC + STEP_C[delta]


def turn(value, back=False):
    pairs = []
    for z in range(NZ):
        for y in range(NY):
            for delta in range(NZ):
                owner = ((z + delta) % NZ * NY + y) * ND + z
                d = (z // 2 + STEP_X[delta]) % NX * NC + STEP_C[delta]
                user = (z * NY + y) * ND + d
                pairs.append((user, owner) if back else (owner, user))
    return lax.ppermute(value, ALL, pairs)


def shift_y(value, k):
    return lax.ppermute(value, "y", [(i, (i + k) % NY) for i in range(NY)])


def shift_z(value, k):
    return lax.ppermute(value, "z", [(i, (i + k) % NZ) for i in range(NZ)])


def ring_z(own):
    up1 = shift_z(own, 1)
    down1 = shift_z(own, -1)
    up2 = shift_z(up1, 1)
    down2 = shift_z(down1, -1)
    up3 = shift_z(up2, 1)
    down3 = shift_z(down2, -1)
    up4 = shift_z(up3, 1)
    return [own, up1, up2, up3, up4, down3, down2, down1]


def two_halves(value):
    high = value.astype(bf16)
    low = (value - high.astype(f32)).astype(bf16)
    return high, low


def pack_kernel(w_in, w_val, w_gate, out, row, sems):
    copies = [
        pltpu.make_async_copy(ref.at[0], row.at[:, pl.ds(i * COLS, COLS)], sems.at[i])
        for i, ref in enumerate((w_in, w_val, w_gate))
    ]
    for copy in copies:
        copy.start()
    for copy in copies:
        copy.wait()
    for i in range(NZ):
        out[i] = row[...]


def prep_kernel(
    lam_re,
    lam_im,
    log_dt,
    b_re,
    b_im,
    r_re,
    r_im,
    d_skip,
    state,
    w_in,
    w_val,
    w_gate,
    base,
    drive,
    carried,
    late,
):
    groups, chans, half = b_re.shape[1:]
    size = groups * chans
    row = lax.broadcasted_iota(jnp.int32, (size, size), 0)
    col = lax.broadcasted_iota(jnp.int32, (size, size), 1)
    for n in range(LAYERS):
        steps = jnp.concatenate([jnp.full((1, half), log_dt[n, g], f32) for g in range(groups)])
        step = jnp.exp(steps)
        re, im = lam_re[n], lam_im[n]
        decay = jnp.exp(re * step)
        angle = im * step
        keep_re = decay * jnp.cos(angle)
        keep_im = decay * jnp.sin(angle)
        denom = re * re + im * im
        ratio_re = ((keep_re - 1.0) * re + keep_im * im) / denom
        ratio_im = (keep_im * re - (keep_re - 1.0) * im) / denom
        drives, reads, offsets = [], [], []
        for g in range(groups):
            q_re, q_im = ratio_re[g : g + 1], ratio_im[g : g + 1]
            d_re = q_re * b_re[n, g] - q_im * b_im[n, g]
            d_im = q_re * b_im[n, g] + q_im * b_re[n, g]
            drives.append(jnp.concatenate([d_re, d_im], axis=1))
            reads.append(jnp.concatenate([r_re[n, g], -r_im[n, g]], axis=1))
            k_re, k_im = keep_re[g : g + 1], keep_im[g : g + 1]
            old = state[n, :, g, :]
            swapped = jnp.concatenate([old[:, half:], old[:, :half]], axis=1)
            new = (
                jnp.concatenate([k_re, k_re], axis=1) * old
                + jnp.concatenate([-k_im, k_im], axis=1) * swapped
            )
            base[n, :, g, :] = new
            offsets.append(times_turned(new, reads[g], HIGHEST))
        dcat = jnp.concatenate(drives)
        drive[n] = dcat
        full = times_turned(dcat, jnp.concatenate(reads), HIGHEST)
        mix = jnp.where(row // chans == col // chans, full, 0.0)
        mix = mix + jnp.where(row == col, d_skip[n : n + 1, :], 0.0)
        carried[n * SEQS : (n + 1) * SEQS, :] = jnp.concatenate(offsets, axis=1)
        if n == 0:
            carried[LAYERS * SEQS :, :] = mix
        else:
            late[...] = jnp.concatenate([w_val[n], w_gate[n], w_in[n], *two_halves(mix)], axis=1)


def write_payload(pay_ref, x, blocks, offset, mix=None):
    squares = jnp.sum(x * x, axis=1, keepdims=True)
    s_high, s_low = two_halves(squares)
    lane = lax.broadcasted_iota(jnp.int32, (SEQS, 128), 1)
    s_part = jnp.where(lane == 0, s_high.astype(f32), jnp.where(lane == 1, s_low.astype(f32), 0.0))
    parts = [blocks[j].astype(bf16) for j in range(NZ)]
    parts += [*two_halves(offset), s_part.astype(bf16)]
    if mix is not None:
        half = BLOCK // 2
        for m in two_halves(mix):
            parts += [m[:half], m[half:]]
    row = jnp.concatenate(parts, axis=1)
    for i in range(ND):
        pay_ref[i] = row


def times_turned(left, right, precision=None):
    return lax.dot_general(
        left, right, (((1,), (1,)), ((), ())), precision=precision, preferred_element_type=f32
    )


def first_kernel(p0, p1, p2, p3, gain, carried, w, up, down, pay_ref, x_ref, rows):
    y = lax.axis_index("y")
    for k, piece in enumerate((p0, p1, p2, p3)):
        rows[lax.rem(y + NY - k, NY)] = piece[...].astype(f32)
    x = rows[...].reshape(SEQS, COLS)
    x_ref[...] = x
    normed = (x * gain[0:1]).astype(bf16)
    blocks = [times_turned(normed, w[j, :, :COLS]) for j in range(NZ)]
    write_payload(pay_ref, x, blocks, carried[:SEQS], carried[LAYERS * SEQS :])


def next_kernel(out, r1, r2, r3, x_old, gain, carried, *refs):
    w = refs[:NZ]
    pay_ref, x_ref, blocks = refs[NZ:]
    z = lax.axis_index("z")
    total = out[...] + r1[...] + r2[...] + r3[...]
    x = x_old[...] + total[:, :COLS] * jax.nn.sigmoid(total[:, COLS:])
    x = x.astype(bf16).astype(f32)
    x_ref[...] = x
    normed = (x * gain[1:2]).astype(bf16)
    for k in range(NZ):
        blocks[lax.rem(z + NZ - k, NZ)] = times_turned(normed, w[k][:, 2 * COLS : 3 * COLS])
    write_payload(pay_ref, x, blocks, carried[SEQS : LAYERS * SEQS])


def inputs_of(got):
    total = got[0, :, :WIDTH].astype(f32)
    squares = got[0, :, WIDTH + 128 : WIDTH + 256].astype(f32)
    for i in range(1, ND):
        total = total + got[i, :, :WIDTH].astype(f32)
        squares = squares + got[i, :, WIDTH + 128 : WIDTH + 256].astype(f32)
    return total * lax.rsqrt(jnp.sum(squares, axis=1, keepdims=True) / D + eps)


def gated(got, u_blocks, w, ordered, weights):
    z = lax.axis_index("z")
    for delta in range(NZ):
        block, slot, source = lax.rem(z + delta, NZ), (NZ - delta) % NZ, place(z, delta)
        sent = got[source]
        offset = sent[:, WIDTH : WIDTH + BLOCK].astype(f32)
        offset = offset + sent[:, WIDTH + BLOCK : WIDTH + 2 * BLOCK].astype(f32)
        cut = slice(slot * BLOCK, (slot + 1) * BLOCK)
        if isinstance(w, list):
            m_high = w[slot][:, 3 * COLS : 3 * COLS + BLOCK]
            m_low = w[slot][:, 3 * COLS + BLOCK :]
            weights[cut, :] = w[slot][:, : 2 * COLS]
        else:
            m = sent[:, WIDTH + 256 :]
            m_high = jnp.concatenate([m[:, :BLOCK], m[:, BLOCK : 2 * BLOCK]], axis=0)
            m_low = jnp.concatenate([m[:, 2 * BLOCK : 3 * BLOCK], m[:, 3 * BLOCK :]], axis=0)
            weights[cut, :] = w[block][:, COLS:]
        high, low = two_halves(u_blocks[block])
        pre = (
            offset
            + jnp.dot(high, m_low, preferred_element_type=f32)
            + jnp.dot(low, m_high, preferred_element_type=f32)
            + jnp.dot(high, m_high, preferred_element_type=f32)
        )
        ordered[:, cut] = jax.nn.gelu(pre).astype(bf16)
    return jnp.dot(ordered[...], weights[...], preferred_element_type=f32)


def own_block(u_blocks):
    z = lax.axis_index("z")
    d = lax.axis_index("x") * NC + lax.axis_index("c")
    delta = jnp.int32(0)
    for other in range(1, NZ):
        delta = jnp.where(place(z, other) == d, other, delta)
    return u_blocks[lax.rem(z + delta, NZ)]


def split_blocks(u, u_blocks):
    for j in range(NZ):
        u_blocks[j] = u[:, j * BLOCK : (j + 1) * BLOCK]


def mid_kernel(got, w, out, own_u, u_blocks, ordered, weights):
    split_blocks(inputs_of(got), u_blocks)
    own_u[...] = own_block(u_blocks)
    out[...] = gated(got, u_blocks, w, ordered, weights)


def inputs_kernel(got, earlier, u_blocks, own_u):
    split_blocks(inputs_of(got), u_blocks)
    own_u[...] = own_block(u_blocks)


def last_kernel(got, u_blocks, *refs):
    w = list(refs[:NZ])
    own_out, s1, s2, s3, ordered, weights, by_y = refs[NZ:]
    out = gated(got, u_blocks, w, ordered, weights)
    y = lax.axis_index("y")
    by_y[...] = out.reshape(NY, ROWS, 2 * COLS)
    own_out[...] = by_y[y]
    for k, ref in enumerate((s1, s2, s3), 1):
        ref[...] = by_y[lax.rem(y + k, NY)]


def stream_kernel(own, r1, r2, r3, x, out):
    y = lax.axis_index("y")
    total = own[...] + r1[...] + r2[...] + r3[...]
    mine = x[pl.ds(pl.multiple_of(y * ROWS, ROWS), ROWS), :]
    out[...] = (mine + total[:, :COLS] * jax.nn.sigmoid(total[:, COLS:])).astype(bf16)


def states_kernel(base, drive, u0, u1, out):
    groups = base.shape[2]
    chans = BLOCK // groups
    for n, u in enumerate((u0, u1)):
        for g in range(groups):
            cut = slice(g * chans, (g + 1) * chans)
            push = jnp.dot(u[:, cut], drive[n, cut, :], precision=HIGHEST, preferred_element_type=f32)
            out[n, :, g, :] = base[n, :, g, :] + push


def call(body, args, outs, scratch=(), scalar=None, space=pltpu.VMEM):
    spaces = [pltpu.SMEM if i == scalar else space for i in range(len(args))]
    return pl.pallas_call(
        body,
        in_specs=[pl.BlockSpec(memory_space=s) for s in spaces],
        out_specs=[pl.BlockSpec(memory_space=pltpu.VMEM) for _ in outs],
        out_shape=outs,
        scratch_shapes=list(scratch),
        compiler_params=pltpu.CompilerParams(vmem_limit_bytes=(60 if space is pl.ANY else 12) << 20),
        cost_estimate=pl.CostEstimate(flops=1 << 24, bytes_accessed=1 << 20, transcendentals=0),
    )(*args)


def shape(dims, dtype=f32):
    return jax.ShapeDtypeStruct(dims, dtype)


FIRST_PAY = WIDTH + 512
NEXT_PAY = WIDTH + 256
BLOCKS = pltpu.VMEM((NZ, SEQS, BLOCK), f32)
GATED = [pltpu.VMEM((SEQS, WIDTH), bf16), pltpu.VMEM((WIDTH, 2 * COLS), bf16)]


def both_layers(
    stream,
    norm_gain,
    w_input,
    lam_re,
    lam_im,
    log_dt,
    b_re,
    b_im,
    readout_real,
    readout_imaginary,
    d_skip,
    w_val,
    w_gate,
    state,
):
    w_turned = jnp.swapaxes(w_input, 1, 2)
    (packed,) = call(
        pack_kernel,
        [w_turned, w_val, w_gate],
        [shape((NZ, BLOCK, 3 * COLS), bf16)],
        [pltpu.VMEM((BLOCK, 3 * COLS), bf16), pltpu.SemaphoreType.DMA((3,))],
        space=pl.ANY,
    )
    first_w = lax.all_to_all(packed, "z", 0, 0, tiled=True)
    pieces = [stream] + [shift_y(stream, k) for k in range(1, NY)]
    base, drive, own, late = call(
        prep_kernel,
        [
            lam_re,
            lam_im,
            log_dt,
            jnp.swapaxes(b_re, 2, 3),
            jnp.swapaxes(b_im, 2, 3),
            readout_real,
            readout_imaginary,
            d_skip,
            state,
            w_turned,
            w_val,
            w_gate,
        ],
        [
            shape(state.shape),
            shape((LAYERS, BLOCK, state.shape[-1])),
            shape((LAYERS * SEQS + BLOCK, BLOCK)),
            shape((BLOCK, 3 * COLS + 2 * BLOCK), bf16),
        ],
        scalar=2,
    )
    carried = turn(own)
    ring = ring_z(late)

    payload, x = call(
        first_kernel,
        [*pieces, norm_gain, carried, first_w, ring[1], ring[-1]],
        [shape((ND, SEQS, FIRST_PAY), bf16), shape((SEQS, COLS))],
        [pltpu.VMEM((NY, ROWS, COLS), f32)],
    )
    got = lax.all_to_all(payload, DP, 0, 0, tiled=True)
    out, u0 = call(
        mid_kernel,
        [got, first_w],
        [shape((SEQS, 2 * COLS)), shape((SEQS, BLOCK))],
        [BLOCKS, *GATED],
    )
    others = [shift_y(out, k) for k in range(1, NY)]
    u0 = turn(u0, back=True)
    payload, x = call(
        next_kernel,
        [out, *others, x, norm_gain, carried, *ring],
        [shape((ND, SEQS, NEXT_PAY), bf16), shape((SEQS, COLS))],
        [BLOCKS],
    )
    got = lax.all_to_all(payload, DP, 0, 0, tiled=True)
    u, u1 = call(
        inputs_kernel, [got, u0], [shape((NZ, SEQS, BLOCK)), shape((SEQS, BLOCK))]
    )
    u1 = turn(u1, back=True)
    own, s1, s2, s3 = call(
        last_kernel,
        [got, u, *ring],
        [shape((ROWS, 2 * COLS))] * NY,
        [*GATED, pltpu.VMEM((NY, ROWS, 2 * COLS), f32)],
    )
    others = [shift_y(sent, k) for k, sent in enumerate((s1, s2, s3), 1)]
    (stream,) = call(stream_kernel, [own, *others, x], [shape((ROWS, COLS), bf16)])
    (states,) = call(states_kernel, [base, drive, u0, u1], [shape(state.shape)])
    return (stream, states)


def solution(mesh):
    grid = Mesh(mesh.devices.reshape(NZ, NY, NX, NC), ALL)
    return jax.shard_map(
        both_layers,
        mesh=grid,
        in_specs=(
            P(TP, DP),
            P(None, DP),
            P(None, DP, TP),
            P(None, TP, None),
            P(None, TP, None),
            P(None, TP),
            P(None, TP, None, None),
            P(None, TP, None, None),
            P(None, TP, None, None),
            P(None, TP, None, None),
            P(None, TP),
            P(None, TP, DP),
            P(None, TP, DP),
            P(None, DP, TP, None),
        ),
        out_specs=(P(TP, DP), P(None, DP, TP, None)),
        check_vma=False,
    )
```

```python
import jax
import jax.numpy as jnp
from jax import lax
from jax.experimental import pallas as pl
from jax.experimental.pallas import tpu as pltpu
from jax.sharding import Mesh
from jax.sharding import PartitionSpec as P

D = 2048
LAYERS = 2
NZ, NY, NX, NC = 8, 4, 4, 2
ND = NX * NC
TP = ("z", "y")
DP = ("x", "c")
ALL = ("z", "y", "x", "c")
ROWS = 8
SEQS = NY * ROWS
COLS = 256
BLOCK = 64
WIDTH = NZ * BLOCK

eps = 1e-06
HIGHEST = lax.Precision.HIGHEST
f32 = jnp.float32
bf16 = jnp.bfloat16


STEP_X = (2, 3, 1, 0, 0, 1, 3, 2)
STEP_C = (1, 1, 1, 1, 0, 0, 0, 0)


def place(z, delta):
    return lax.rem(lax.div(z, 2) + STEP_X[delta], NX) * NC + STEP_C[delta]


def turn(value, back=False):
    pairs = []
    for z in range(NZ):
        for y in range(NY):
            for delta in range(NZ):
                owner = ((z + delta) % NZ * NY + y) * ND + z
                d = (z // 2 + STEP_X[delta]) % NX * NC + STEP_C[delta]
                user = (z * NY + y) * ND + d
                pairs.append((user, owner) if back else (owner, user))
    return lax.ppermute(value, ALL, pairs)


def shift_y(value, k):
    return lax.ppermute(value, "y", [(i, (i + k) % NY) for i in range(NY)])


def shift_z(value, k):
    return lax.ppermute(value, "z", [(i, (i + k) % NZ) for i in range(NZ)])


def ring_z(own):
    ups, downs = [own], [own]
    for step in range(1, NZ // 2 + 1):
        ups.append(shift_z(ups[-1], 1))
        if step < NZ // 2:
            downs.append(shift_z(downs[-1], -1))
    return ups + downs[:0:-1]


def two_halves(value):
    high = value.astype(bf16)
    low = (value - high.astype(f32)).astype(bf16)
    return high, low


def pack_kernel(w_in, w_val, w_gate, out, soon, first, row, sems):
    parts = [(w_in.at[0], first), (w_val.at[0], row.at[:, pl.ds(0, COLS)])]
    parts += [(w_gate.at[0], row.at[:, pl.ds(COLS, COLS)])]
    parts += [(w_in.at[1], row.at[:, pl.ds(2 * COLS, COLS)])]
    copies = [pltpu.make_async_copy(a, b, sems.at[i]) for i, (a, b) in enumerate(parts)]
    for copy in copies:
        copy.start()
    for copy in copies:
        copy.wait()
    for i in range(NZ):
        out[i] = first[...]
    soon[...] = row[...]


def prep_kernel(
    lam_re,
    lam_im,
    log_dt,
    b_re,
    b_im,
    r_re,
    r_im,
    d_skip,
    state,
    w_val,
    w_gate,
    base,
    drive,
    carried,
    late,
):
    groups, chans, half = b_re.shape[1:]
    size = groups * chans
    row = lax.broadcasted_iota(jnp.int32, (size, size), 0)
    col = lax.broadcasted_iota(jnp.int32, (size, size), 1)
    for n in range(LAYERS):
        steps = jnp.concatenate([jnp.full((1, half), log_dt[n, g], f32) for g in range(groups)])
        step = jnp.exp(steps)
        re, im = lam_re[n], lam_im[n]
        decay = jnp.exp(re * step)
        angle = im * step
        keep_re = decay * jnp.cos(angle)
        keep_im = decay * jnp.sin(angle)
        denom = re * re + im * im
        ratio_re = ((keep_re - 1.0) * re + keep_im * im) / denom
        ratio_im = (keep_im * re - (keep_re - 1.0) * im) / denom
        drives, reads, offsets = [], [], []
        for g in range(groups):
            q_re, q_im = ratio_re[g : g + 1], ratio_im[g : g + 1]
            d_re = q_re * b_re[n, g] - q_im * b_im[n, g]
            d_im = q_re * b_im[n, g] + q_im * b_re[n, g]
            drives.append(jnp.concatenate([d_re, d_im], axis=1))
            reads.append(jnp.concatenate([r_re[n, g], -r_im[n, g]], axis=1))
            k_re, k_im = keep_re[g : g + 1], keep_im[g : g + 1]
            old = state[n, :, g, :]
            swapped = jnp.concatenate([old[:, half:], old[:, :half]], axis=1)
            new = (
                jnp.concatenate([k_re, k_re], axis=1) * old
                + jnp.concatenate([-k_im, k_im], axis=1) * swapped
            )
            base[n, :, g, :] = new
            offsets.append(times_turned(new, reads[g], HIGHEST))
        dcat = jnp.concatenate(drives)
        drive[n] = dcat
        full = times_turned(dcat, jnp.concatenate(reads), HIGHEST)
        mix = jnp.where(row // chans == col // chans, full, 0.0)
        mix = mix + jnp.where(row == col, d_skip[n : n + 1, :], 0.0)
        carried[n * SEQS : (n + 1) * SEQS, :] = jnp.concatenate(offsets, axis=1)
        if n == 0:
            carried[LAYERS * SEQS :, :] = mix
        else:
            late[...] = jnp.concatenate([w_val[n], w_gate[n], *two_halves(mix)], axis=1)


def write_payload(pay_ref, x, blocks, offset, mix=None):
    squares = jnp.sum(x * x, axis=1, keepdims=True)
    s_high, s_low = two_halves(squares)
    lane = lax.broadcasted_iota(jnp.int32, (SEQS, 128), 1)
    s_part = jnp.where(lane == 0, s_high.astype(f32), jnp.where(lane == 1, s_low.astype(f32), 0.0))
    parts = [blocks[j].astype(bf16) for j in range(NZ)]
    parts += [*two_halves(offset), s_part.astype(bf16)]
    if mix is not None:
        half = BLOCK // 2
        for m in two_halves(mix):
            parts += [m[:half], m[half:]]
    row = jnp.concatenate(parts, axis=1)
    for i in range(ND):
        pay_ref[i] = row


def times_turned(left, right, precision=None):
    return lax.dot_general(
        left, right, (((1,), (1,)), ((), ())), precision=precision, preferred_element_type=f32
    )


def first_kernel(p0, p1, p2, p3, gain, carried, w, pay_ref, x_ref, rows):
    y = lax.axis_index("y")
    for k, piece in enumerate((p0, p1, p2, p3)):
        rows[lax.rem(y + NY - k, NY)] = piece[...].astype(f32)
    x = rows[...].reshape(SEQS, COLS)
    x_ref[...] = x
    normed = (x * gain[0:1]).astype(bf16)
    blocks = [times_turned(normed, w[j]) for j in range(NZ)]
    write_payload(pay_ref, x, blocks, carried[:SEQS], carried[LAYERS * SEQS :])


def next_kernel(out, r1, r2, r3, x_old, gain, carried, *refs):
    w = refs[:NZ]
    pay_ref, x_ref, blocks = refs[NZ:]
    z = lax.axis_index("z")
    total = out[...] + r1[...] + r2[...] + r3[...]
    x = x_old[...] + total[:, :COLS] * jax.nn.sigmoid(total[:, COLS:])
    x = x.astype(bf16).astype(f32)
    x_ref[...] = x
    normed = (x * gain[1:2]).astype(bf16)
    for k in range(NZ):
        blocks[lax.rem(z + NZ - k, NZ)] = times_turned(normed, w[k][:, 2 * COLS : 3 * COLS])
    write_payload(pay_ref, x, blocks, carried[SEQS : LAYERS * SEQS])


def inputs_of(got):
    total = got[0, :, :WIDTH].astype(f32)
    squares = got[0, :, WIDTH + 128 : WIDTH + 256].astype(f32)
    for i in range(1, ND):
        total = total + got[i, :, :WIDTH].astype(f32)
        squares = squares + got[i, :, WIDTH + 128 : WIDTH + 256].astype(f32)
    return total * lax.rsqrt(jnp.sum(squares, axis=1, keepdims=True) / D + eps)


def gated(got, u_blocks, w, ordered, weights):
    z = lax.axis_index("z")
    for delta in range(NZ):
        block, slot, source = lax.rem(z + delta, NZ), (NZ - delta) % NZ, place(z, delta)
        sent = got[source]
        offset = sent[:, WIDTH : WIDTH + BLOCK].astype(f32)
        offset = offset + sent[:, WIDTH + BLOCK : WIDTH + 2 * BLOCK].astype(f32)
        cut = slice(slot * BLOCK, (slot + 1) * BLOCK)
        weights[cut, :] = w[slot][:, : 2 * COLS]
        if got.shape[2] == NEXT_PAY:
            m_high = w[slot][:, 2 * COLS : 2 * COLS + BLOCK]
            m_low = w[slot][:, 2 * COLS + BLOCK :]
        else:
            m = sent[:, WIDTH + 256 :]
            m_high = jnp.concatenate([m[:, :BLOCK], m[:, BLOCK : 2 * BLOCK]], axis=0)
            m_low = jnp.concatenate([m[:, 2 * BLOCK : 3 * BLOCK], m[:, 3 * BLOCK :]], axis=0)
        high, low = two_halves(u_blocks[block])
        pre = (
            offset
            + jnp.dot(high, m_low, preferred_element_type=f32)
            + jnp.dot(low, m_high, preferred_element_type=f32)
            + jnp.dot(high, m_high, preferred_element_type=f32)
        )
        ordered[:, cut] = jax.nn.gelu(pre).astype(bf16)
    return jnp.dot(ordered[...], weights[...], preferred_element_type=f32)


def own_block(u_blocks):
    z = lax.axis_index("z")
    d = lax.axis_index("x") * NC + lax.axis_index("c")
    delta = jnp.int32(0)
    for other in range(1, NZ):
        delta = jnp.where(place(z, other) == d, other, delta)
    return u_blocks[lax.rem(z + delta, NZ)]


def split_blocks(u, u_blocks):
    for j in range(NZ):
        u_blocks[j] = u[:, j * BLOCK : (j + 1) * BLOCK]


def mid_kernel(got, *refs):
    w = refs[:NZ]
    out, own_u, u_blocks, ordered, weights = refs[NZ:]
    split_blocks(inputs_of(got), u_blocks)
    own_u[...] = own_block(u_blocks)
    out[...] = gated(got, u_blocks, w, ordered, weights)


def inputs_kernel(got, earlier, u_blocks, own_u):
    split_blocks(inputs_of(got), u_blocks)
    own_u[...] = own_block(u_blocks)


def last_kernel(got, u_blocks, *refs):
    w = refs[:NZ]
    own_out, s1, s2, s3, ordered, weights, by_y = refs[NZ:]
    out = gated(got, u_blocks, w, ordered, weights)
    y = lax.axis_index("y")
    by_y[...] = out.reshape(NY, ROWS, 2 * COLS)
    own_out[...] = by_y[y]
    for k, ref in enumerate((s1, s2, s3), 1):
        ref[...] = by_y[lax.rem(y + k, NY)]


def stream_kernel(own, r1, r2, r3, x, out):
    y = lax.axis_index("y")
    total = own[...] + r1[...] + r2[...] + r3[...]
    mine = x[pl.ds(pl.multiple_of(y * ROWS, ROWS), ROWS), :]
    out[...] = (mine + total[:, :COLS] * jax.nn.sigmoid(total[:, COLS:])).astype(bf16)


def states_kernel(base, drive, u0, u1, out):
    groups = base.shape[2]
    chans = BLOCK // groups
    for n, u in enumerate((u0, u1)):
        for g in range(groups):
            cut = slice(g * chans, (g + 1) * chans)
            push = jnp.dot(u[:, cut], drive[n, cut, :], precision=HIGHEST, preferred_element_type=f32)
            out[n, :, g, :] = base[n, :, g, :] + push


def call(body, args, outs, scratch=(), scalar=None, space=pltpu.VMEM):
    spaces = [pltpu.SMEM if i == scalar else space for i in range(len(args))]
    return pl.pallas_call(
        body,
        in_specs=[pl.BlockSpec(memory_space=s) for s in spaces],
        out_specs=[pl.BlockSpec(memory_space=pltpu.VMEM) for _ in outs],
        out_shape=outs,
        scratch_shapes=list(scratch),
        compiler_params=pltpu.CompilerParams(vmem_limit_bytes=(60 if space is pl.ANY else 12) << 20),
        cost_estimate=pl.CostEstimate(flops=1 << 24, bytes_accessed=1 << 20, transcendentals=0),
    )(*args)


def shape(dims, dtype=f32):
    return jax.ShapeDtypeStruct(dims, dtype)


FIRST_PAY = WIDTH + 512
NEXT_PAY = WIDTH + 256
BLOCKS = pltpu.VMEM((NZ, SEQS, BLOCK), f32)
GATED = [pltpu.VMEM((SEQS, WIDTH), bf16), pltpu.VMEM((WIDTH, 2 * COLS), bf16)]


def both_layers(
    stream,
    norm_gain,
    w_input,
    lam_re,
    lam_im,
    log_dt,
    b_re,
    b_im,
    readout_real,
    readout_imaginary,
    d_skip,
    w_val,
    w_gate,
    state,
):
    w_turned = jnp.swapaxes(w_input, 1, 2)
    packed, soon = call(
        pack_kernel,
        [w_turned, w_val, w_gate],
        [shape((NZ, BLOCK, COLS), bf16), shape((BLOCK, 3 * COLS), bf16)],
        [
            pltpu.VMEM((BLOCK, COLS), bf16),
            pltpu.VMEM((BLOCK, 3 * COLS), bf16),
            pltpu.SemaphoreType.DMA((4,)),
        ],
        space=pl.ANY,
    )
    first_w = lax.all_to_all(packed, "z", 0, 0, tiled=True)
    pieces = [stream] + [shift_y(stream, k) for k in range(1, NY)]
    base, drive, own, late = call(
        prep_kernel,
        [
            lam_re,
            lam_im,
            log_dt,
            jnp.swapaxes(b_re, 2, 3),
            jnp.swapaxes(b_im, 2, 3),
            readout_real,
            readout_imaginary,
            d_skip,
            state,
            w_val,
            w_gate,
        ],
        [
            shape(state.shape),
            shape((LAYERS, BLOCK, state.shape[-1])),
            shape((LAYERS * SEQS + BLOCK, BLOCK)),
            shape((BLOCK, 2 * COLS + 2 * BLOCK), bf16),
        ],
        scalar=2,
    )
    carried = turn(own)
    ring_soon = ring_z(soon)
    ring_late = ring_z(late)

    payload, x = call(
        first_kernel,
        [*pieces, norm_gain, carried, first_w],
        [shape((ND, SEQS, FIRST_PAY), bf16), shape((SEQS, COLS))],
        [pltpu.VMEM((NY, ROWS, COLS), f32)],
    )
    got = lax.all_to_all(payload, DP, 0, 0, tiled=True)
    out, u0 = call(
        mid_kernel,
        [got, *ring_soon],
        [shape((SEQS, 2 * COLS)), shape((SEQS, BLOCK))],
        [BLOCKS, *GATED],
    )
    others = [shift_y(out, k) for k in range(1, NY)]
    u0 = turn(u0, back=True)
    payload, x = call(
        next_kernel,
        [out, *others, x, norm_gain, carried, *ring_soon],
        [shape((ND, SEQS, NEXT_PAY), bf16), shape((SEQS, COLS))],
        [BLOCKS],
    )
    got = lax.all_to_all(payload, DP, 0, 0, tiled=True)
    u, u1 = call(
        inputs_kernel, [got, u0], [shape((NZ, SEQS, BLOCK)), shape((SEQS, BLOCK))]
    )
    u1 = turn(u1, back=True)
    own, s1, s2, s3 = call(
        last_kernel,
        [got, u, *ring_late],
        [shape((ROWS, 2 * COLS))] * NY,
        [*GATED, pltpu.VMEM((NY, ROWS, 2 * COLS), f32)],
    )
    others = [shift_y(sent, k) for k, sent in enumerate((s1, s2, s3), 1)]
    (stream,) = call(stream_kernel, [own, *others, x], [shape((ROWS, COLS), bf16)])
    (states,) = call(states_kernel, [base, drive, u0, u1], [shape(state.shape)])
    return (stream, states)


def solution(mesh):
    grid = Mesh(mesh.devices.reshape(NZ, NY, NX, NC), ALL)
    return jax.shard_map(
        both_layers,
        mesh=grid,
        in_specs=(
            P(TP, DP),
            P(None, DP),
            P(None, DP, TP),
            P(None, TP, None),
            P(None, TP, None),
            P(None, TP),
            P(None, TP, None, None),
            P(None, TP, None, None),
            P(None, TP, None, None),
            P(None, TP, None, None),
            P(None, TP),
            P(None, TP, DP),
            P(None, TP, DP),
            P(None, DP, TP, None),
        ),
        out_specs=(P(TP, DP), P(None, DP, TP, None)),
        check_vma=False,
    )
```

```python
import jax
import jax.numpy as jnp
from jax import lax
from jax.experimental import pallas as pl
from jax.experimental.pallas import tpu as pltpu
from jax.sharding import Mesh
from jax.sharding import PartitionSpec as P

D = 2048
LAYERS = 2
NZ, NY, NX, NC = 8, 4, 4, 2
ND = NX * NC
TP = ("z", "y")
DP = ("x", "c")
ALL = ("z", "y", "x", "c")
ROWS = 8
SEQS = NY * ROWS
COLS = 256
BLOCK = 64
WIDTH = NZ * BLOCK

eps = 1e-06
HIGHEST = lax.Precision.HIGHEST
f32 = jnp.float32
bf16 = jnp.bfloat16


STEP_X = (2, 3, 1, 0, 0, 1, 3, 2)
STEP_C = (1, 1, 1, 1, 0, 0, 0, 0)


def place(z, delta):
    return lax.rem(lax.div(z, 2) + STEP_X[delta], NX) * NC + STEP_C[delta]


def turn(value, back=False):
    pairs = []
    for z in range(NZ):
        for y in range(NY):
            for delta in range(NZ):
                owner = ((z + delta) % NZ * NY + y) * ND + z
                d = (z // 2 + STEP_X[delta]) % NX * NC + STEP_C[delta]
                user = (z * NY + y) * ND + d
                pairs.append((user, owner) if back else (owner, user))
    return lax.ppermute(value, ALL, pairs)


def shift_y(value, k):
    return lax.ppermute(value, "y", [(i, (i + k) % NY) for i in range(NY)])


def shift_z(value, k):
    return lax.ppermute(value, "z", [(i, (i + k) % NZ) for i in range(NZ)])


def ring_z(own):
    ups, downs = [own], [own]
    for step in range(1, NZ // 2 + 1):
        ups.append(shift_z(ups[-1], 1))
        if step < NZ // 2:
            downs.append(shift_z(downs[-1], -1))
    return ups + downs[:0:-1]


def two_halves(value):
    high = value.astype(bf16)
    low = (value - high.astype(f32)).astype(bf16)
    return high, low


def pack_kernel(w_in, w_val, w_gate, out, soon, first, row, sems):
    parts = [(w_in.at[0], first), (w_val.at[0], row.at[:, pl.ds(0, COLS)])]
    parts += [(w_gate.at[0], row.at[:, pl.ds(COLS, COLS)])]
    parts += [(w_in.at[1], row.at[:, pl.ds(2 * COLS, COLS)])]
    copies = [pltpu.make_async_copy(a, b, sems.at[i]) for i, (a, b) in enumerate(parts)]
    for copy in copies:
        copy.start()
    for copy in copies:
        copy.wait()
    for i in range(NZ):
        out[i] = first[...]
    soon[...] = row[...]


def prep_kernel(
    lam_re,
    lam_im,
    log_dt,
    b_re,
    b_im,
    r_re,
    r_im,
    d_skip,
    state,
    w_val,
    w_gate,
    base,
    drive,
    carried,
    late,
):
    groups, chans, half = b_re.shape[1:]
    size = groups * chans
    row = lax.broadcasted_iota(jnp.int32, (size, size), 0)
    col = lax.broadcasted_iota(jnp.int32, (size, size), 1)
    for n in range(LAYERS):
        steps = jnp.concatenate([jnp.full((1, half), log_dt[n, g], f32) for g in range(groups)])
        step = jnp.exp(steps)
        re, im = lam_re[n], lam_im[n]
        decay = jnp.exp(re * step)
        angle = im * step
        keep_re = decay * jnp.cos(angle)
        keep_im = decay * jnp.sin(angle)
        denom = re * re + im * im
        ratio_re = ((keep_re - 1.0) * re + keep_im * im) / denom
        ratio_im = (keep_im * re - (keep_re - 1.0) * im) / denom
        drives, reads, offsets = [], [], []
        for g in range(groups):
            q_re, q_im = ratio_re[g : g + 1], ratio_im[g : g + 1]
            d_re = q_re * b_re[n, g] - q_im * b_im[n, g]
            d_im = q_re * b_im[n, g] + q_im * b_re[n, g]
            drives.append(jnp.concatenate([d_re, d_im], axis=1))
            reads.append(jnp.concatenate([r_re[n, g], -r_im[n, g]], axis=1))
            k_re, k_im = keep_re[g : g + 1], keep_im[g : g + 1]
            old = state[n, :, g, :]
            swapped = jnp.concatenate([old[:, half:], old[:, :half]], axis=1)
            new = (
                jnp.concatenate([k_re, k_re], axis=1) * old
                + jnp.concatenate([-k_im, k_im], axis=1) * swapped
            )
            base[n, :, g, :] = new
            offsets.append(times_turned(new, reads[g], HIGHEST))
        dcat = jnp.concatenate(drives)
        drive[n] = dcat
        full = times_turned(dcat, jnp.concatenate(reads), HIGHEST)
        mix = jnp.where(row // chans == col // chans, full, 0.0)
        mix = mix + jnp.where(row == col, d_skip[n : n + 1, :], 0.0)
        carried[n * SEQS : (n + 1) * SEQS, :] = jnp.concatenate(offsets, axis=1)
        if n == 0:
            carried[LAYERS * SEQS :, :] = mix
        else:
            late[...] = jnp.concatenate([w_val[n], w_gate[n], *two_halves(mix)], axis=1)


def write_payload(pay_ref, x, blocks, offset, mix=None):
    squares = jnp.sum(x * x, axis=1, keepdims=True)
    s_high, s_low = two_halves(squares)
    lane = lax.broadcasted_iota(jnp.int32, (SEQS, 128), 1)
    s_part = jnp.where(lane == 0, s_high.astype(f32), jnp.where(lane == 1, s_low.astype(f32), 0.0))
    parts = [blocks[j].astype(bf16) for j in range(NZ)]
    parts += [*two_halves(offset), s_part.astype(bf16)]
    if mix is not None:
        half = BLOCK // 2
        for m in two_halves(mix):
            parts += [m[:half], m[half:]]
    row = jnp.concatenate(parts, axis=1)
    for i in range(ND):
        pay_ref[i] = row


def times_turned(left, right, precision=None):
    return lax.dot_general(
        left, right, (((1,), (1,)), ((), ())), precision=precision, preferred_element_type=f32
    )


def first_kernel(p0, p1, p2, p3, gain, carried, w, pay_ref, x_ref, rows):
    y = lax.axis_index("y")
    for k, piece in enumerate((p0, p1, p2, p3)):
        rows[lax.rem(y + NY - k, NY)] = piece[...].astype(f32)
    x = rows[...].reshape(SEQS, COLS)
    x_ref[...] = x
    normed = (x * gain[0:1]).astype(bf16)
    blocks = [times_turned(normed, w[j]) for j in range(NZ)]
    write_payload(pay_ref, x, blocks, carried[:SEQS], carried[LAYERS * SEQS :])


def next_kernel(out, r1, r2, r3, x_old, gain, carried, *refs):
    w = refs[:NZ]
    pay_ref, x_ref, blocks = refs[NZ:]
    z = lax.axis_index("z")
    total = out[...] + r1[...] + r2[...] + r3[...]
    x = x_old[...] + total[:, :COLS] * jax.nn.sigmoid(total[:, COLS:])
    x = x.astype(bf16).astype(f32)
    x_ref[...] = x
    normed = (x * gain[1:2]).astype(bf16)
    for k in range(NZ):
        blocks[lax.rem(z + NZ - k, NZ)] = times_turned(normed, w[k][:, 2 * COLS : 3 * COLS])
    write_payload(pay_ref, x, blocks, carried[SEQS : LAYERS * SEQS])


def inputs_of(got):
    total = got[0, :, :WIDTH].astype(f32)
    squares = got[0, :, WIDTH + 128 : WIDTH + 256].astype(f32)
    for i in range(1, ND):
        total = total + got[i, :, :WIDTH].astype(f32)
        squares = squares + got[i, :, WIDTH + 128 : WIDTH + 256].astype(f32)
    return total * lax.rsqrt(jnp.sum(squares, axis=1, keepdims=True) / D + eps)


def gated(got, u_blocks, w, ordered, weights):
    z = lax.axis_index("z")
    for delta in range(NZ):
        block, slot, source = lax.rem(z + delta, NZ), (NZ - delta) % NZ, place(z, delta)
        sent = got[source]
        offset = sent[:, WIDTH : WIDTH + BLOCK].astype(f32)
        offset = offset + sent[:, WIDTH + BLOCK : WIDTH + 2 * BLOCK].astype(f32)
        cut = slice(slot * BLOCK, (slot + 1) * BLOCK)
        weights[cut, :] = w[slot][:, : 2 * COLS]
        if got.shape[2] == NEXT_PAY:
            m_high = w[slot][:, 2 * COLS : 2 * COLS + BLOCK]
            m_low = w[slot][:, 2 * COLS + BLOCK :]
        else:
            m = sent[:, WIDTH + 256 :]
            m_high = jnp.concatenate([m[:, :BLOCK], m[:, BLOCK : 2 * BLOCK]], axis=0)
            m_low = jnp.concatenate([m[:, 2 * BLOCK : 3 * BLOCK], m[:, 3 * BLOCK :]], axis=0)
        high, low = two_halves(u_blocks[block])
        pre = (
            offset
            + jnp.dot(high, m_low, preferred_element_type=f32)
            + jnp.dot(low, m_high, preferred_element_type=f32)
            + jnp.dot(high, m_high, preferred_element_type=f32)
        )
        ordered[:, cut] = jax.nn.gelu(pre).astype(bf16)
    return jnp.dot(ordered[...], weights[...], preferred_element_type=f32)


def own_block(u_blocks):
    z = lax.axis_index("z")
    d = lax.axis_index("x") * NC + lax.axis_index("c")
    delta = jnp.int32(0)
    for other in range(1, NZ):
        delta = jnp.where(place(z, other) == d, other, delta)
    return u_blocks[lax.rem(z + delta, NZ)]


def split_blocks(u, u_blocks):
    for j in range(NZ):
        u_blocks[j] = u[:, j * BLOCK : (j + 1) * BLOCK]


def mid_kernel(got, *refs):
    w = refs[:NZ]
    out, own_u, u_blocks, ordered, weights = refs[NZ:]
    split_blocks(inputs_of(got), u_blocks)
    own_u[...] = own_block(u_blocks)
    out[...] = gated(got, u_blocks, w, ordered, weights)


def inputs_kernel(got, u_blocks, own_u):
    split_blocks(inputs_of(got), u_blocks)
    own_u[...] = own_block(u_blocks)


def last_kernel(got, u_blocks, *refs):
    w = refs[:NZ]
    own_out, s1, s2, s3, ordered, weights, by_y = refs[NZ:]
    out = gated(got, u_blocks, w, ordered, weights)
    y = lax.axis_index("y")
    by_y[...] = out.reshape(NY, ROWS, 2 * COLS)
    own_out[...] = by_y[y]
    for k, ref in enumerate((s1, s2, s3), 1):
        ref[...] = by_y[lax.rem(y + k, NY)]


def stream_kernel(own, r1, r2, r3, x, out):
    y = lax.axis_index("y")
    total = own[...] + r1[...] + r2[...] + r3[...]
    mine = x[pl.ds(pl.multiple_of(y * ROWS, ROWS), ROWS), :]
    out[...] = (mine + total[:, :COLS] * jax.nn.sigmoid(total[:, COLS:])).astype(bf16)


def states_kernel(base, drive, u0, u1, out):
    groups = base.shape[2]
    chans = BLOCK // groups
    for n, u in enumerate((u0, u1)):
        for g in range(groups):
            cut = slice(g * chans, (g + 1) * chans)
            push = jnp.dot(u[:, cut], drive[n, cut, :], precision=HIGHEST, preferred_element_type=f32)
            out[n, :, g, :] = base[n, :, g, :] + push


def call(body, args, outs, scratch=(), scalar=None, space=pltpu.VMEM):
    spaces = [pltpu.SMEM if i == scalar else space for i in range(len(args))]
    return pl.pallas_call(
        body,
        in_specs=[pl.BlockSpec(memory_space=s) for s in spaces],
        out_specs=[pl.BlockSpec(memory_space=pltpu.VMEM) for _ in outs],
        out_shape=outs,
        scratch_shapes=list(scratch),
        compiler_params=pltpu.CompilerParams(vmem_limit_bytes=(60 if space is pl.ANY else 12) << 20),
        cost_estimate=pl.CostEstimate(flops=1 << 24, bytes_accessed=1 << 20, transcendentals=0),
    )(*args)


def shape(dims, dtype=f32):
    return jax.ShapeDtypeStruct(dims, dtype)


FIRST_PAY = WIDTH + 512
NEXT_PAY = WIDTH + 256
BLOCKS = pltpu.VMEM((NZ, SEQS, BLOCK), f32)
GATED = [pltpu.VMEM((SEQS, WIDTH), bf16), pltpu.VMEM((WIDTH, 2 * COLS), bf16)]


def both_layers(
    stream,
    norm_gain,
    w_input,
    lam_re,
    lam_im,
    log_dt,
    b_re,
    b_im,
    readout_real,
    readout_imaginary,
    d_skip,
    w_val,
    w_gate,
    state,
):
    w_turned = jnp.swapaxes(w_input, 1, 2)
    packed, soon = call(
        pack_kernel,
        [w_turned, w_val, w_gate],
        [shape((NZ, BLOCK, COLS), bf16), shape((BLOCK, 3 * COLS), bf16)],
        [
            pltpu.VMEM((BLOCK, COLS), bf16),
            pltpu.VMEM((BLOCK, 3 * COLS), bf16),
            pltpu.SemaphoreType.DMA((4,)),
        ],
        space=pl.ANY,
    )
    first_w = lax.all_to_all(packed, "z", 0, 0, tiled=True)
    after, before = shift_y(stream, 1), shift_y(stream, -1)
    pieces = [stream, after, shift_y(after, 1), before]
    base, drive, own, late = call(
        prep_kernel,
        [
            lam_re,
            lam_im,
            log_dt,
            jnp.swapaxes(b_re, 2, 3),
            jnp.swapaxes(b_im, 2, 3),
            readout_real,
            readout_imaginary,
            d_skip,
            state,
            w_val,
            w_gate,
        ],
        [
            shape(state.shape),
            shape((LAYERS, BLOCK, state.shape[-1])),
            shape((LAYERS * SEQS + BLOCK, BLOCK)),
            shape((BLOCK, 2 * COLS + 2 * BLOCK), bf16),
        ],
        scalar=2,
    )
    carried = turn(own)
    ring_soon = ring_z(soon)
    ring_late = ring_z(late)

    payload, x = call(
        first_kernel,
        [*pieces, norm_gain, carried, first_w],
        [shape((ND, SEQS, FIRST_PAY), bf16), shape((SEQS, COLS))],
        [pltpu.VMEM((NY, ROWS, COLS), f32)],
    )
    got = lax.all_to_all(payload, DP, 0, 0, tiled=True)
    out, u0 = call(
        mid_kernel,
        [got, *ring_soon],
        [shape((SEQS, 2 * COLS)), shape((SEQS, BLOCK))],
        [BLOCKS, *GATED],
    )
    others = [shift_y(out, k) for k in range(1, NY)]
    u0 = turn(u0, back=True)
    payload, x = call(
        next_kernel,
        [out, *others, x, norm_gain, carried, *ring_soon],
        [shape((ND, SEQS, NEXT_PAY), bf16), shape((SEQS, COLS))],
        [BLOCKS],
    )
    got = lax.all_to_all(payload, DP, 0, 0, tiled=True)
    u, u1 = call(
        inputs_kernel, [got], [shape((NZ, SEQS, BLOCK)), shape((SEQS, BLOCK))]
    )
    u1 = turn(u1, back=True)
    own, s1, s2, s3 = call(
        last_kernel,
        [got, u, *ring_late],
        [shape((ROWS, 2 * COLS))] * NY,
        [*GATED, pltpu.VMEM((NY, ROWS, 2 * COLS), f32)],
    )
    others = [shift_y(sent, k) for k, sent in enumerate((s1, s2, s3), 1)]
    (stream,) = call(stream_kernel, [own, *others, x], [shape((ROWS, COLS), bf16)])
    (states,) = call(states_kernel, [base, drive, u0, u1], [shape(state.shape)])
    return (stream, states)


def solution(mesh):
    grid = Mesh(mesh.devices.reshape(NZ, NY, NX, NC), ALL)
    return jax.shard_map(
        both_layers,
        mesh=grid,
        in_specs=(
            P(TP, DP),
            P(None, DP),
            P(None, DP, TP),
            P(None, TP, None),
            P(None, TP, None),
            P(None, TP),
            P(None, TP, None, None),
            P(None, TP, None, None),
            P(None, TP, None, None),
            P(None, TP, None, None),
            P(None, TP),
            P(None, TP, DP),
            P(None, TP, DP),
            P(None, DP, TP, None),
        ),
        out_specs=(P(TP, DP), P(None, DP, TP, None)),
        check_vma=False,
    )
```

```python
import jax
import jax.numpy as jnp
from jax import lax
from jax.experimental import pallas as pl
from jax.experimental.pallas import tpu as pltpu
from jax.sharding import Mesh
from jax.sharding import PartitionSpec as P

D = 2048
LAYERS = 2
NZ, NY, NX, NC = 8, 4, 4, 2
ND = NX * NC
TP = ("z", "y")
DP = ("x", "c")
ALL = ("z", "y", "x", "c")
ROWS = 8
SEQS = NY * ROWS
COLS = 256
BLOCK = 64
CHANS = 16
WIDTH = NZ * BLOCK

eps = 1e-06
HIGHEST = lax.Precision.HIGHEST
f32 = jnp.float32
bf16 = jnp.bfloat16


STEP_X = (2, 3, 1, 0, 0, 1, 3, 2)
STEP_C = (1, 1, 1, 1, 0, 0, 0, 0)


def place(z, delta):
    return lax.rem(lax.div(z, 2) + STEP_X[delta], NX) * NC + STEP_C[delta]


def turn(value, back=False):
    pairs = []
    for z in range(NZ):
        for y in range(NY):
            for delta in range(NZ):
                owner = ((z + delta) % NZ * NY + y) * ND + z
                d = (z // 2 + STEP_X[delta]) % NX * NC + STEP_C[delta]
                user = (z * NY + y) * ND + d
                pairs.append((user, owner) if back else (owner, user))
    return lax.ppermute(value, ALL, pairs)


def shift_y(value, k):
    return lax.ppermute(value, "y", [(i, (i + k) % NY) for i in range(NY)])


def shift_z(value, k):
    return lax.ppermute(value, "z", [(i, (i + k) % NZ) for i in range(NZ)])


def ring_z(own):
    ups, downs = [own], [own]
    for step in range(1, NZ // 2 + 1):
        ups.append(shift_z(ups[-1], 1))
        if step < NZ // 2:
            downs.append(shift_z(downs[-1], -1))
    return ups + downs[:0:-1]


def two_halves(value):
    high = value.astype(bf16)
    low = (value - high.astype(f32)).astype(bf16)
    return high, low


def pack_kernel(w_in, w_val, w_gate, out, soon, late, first, row, tail, sems):
    parts = [(w_in.at[0], first), (w_val.at[0], row.at[:, pl.ds(0, COLS)])]
    parts += [(w_gate.at[0], row.at[:, pl.ds(COLS, COLS)])]
    parts += [(w_in.at[1], row.at[:, pl.ds(2 * COLS, COLS)])]
    parts += [(w_val.at[1], tail.at[:, pl.ds(0, COLS)])]
    parts += [(w_gate.at[1], tail.at[:, pl.ds(COLS, COLS)])]
    copies = [pltpu.make_async_copy(a, b, sems.at[i]) for i, (a, b) in enumerate(parts)]
    for copy in copies:
        copy.start()
    for copy in copies:
        copy.wait()
    for i in range(NZ):
        out[i] = first[...]
    soon[...] = row[...]
    late[...] = tail[...]


def prep_kernel(
    lam_re,
    lam_im,
    log_dt,
    b_re,
    b_im,
    r_re,
    r_im,
    d_skip,
    state,
    base,
    drive_high,
    drive_low,
    carried,
):
    groups, chans, half = b_re.shape[1:]
    size = groups * chans
    row = lax.broadcasted_iota(jnp.int32, (size, size), 0)
    col = lax.broadcasted_iota(jnp.int32, (size, size), 1)
    for n in range(LAYERS):
        steps = jnp.concatenate([jnp.full((1, half), log_dt[n, g], f32) for g in range(groups)])
        step = jnp.exp(steps)
        re, im = lam_re[n], lam_im[n]
        decay = jnp.exp(re * step)
        angle = im * step
        keep_re = decay * jnp.cos(angle)
        keep_im = decay * jnp.sin(angle)
        denom = re * re + im * im
        ratio_re = ((keep_re - 1.0) * re + keep_im * im) / denom
        ratio_im = (keep_im * re - (keep_re - 1.0) * im) / denom
        drives, reads, offsets = [], [], []
        for g in range(groups):
            q_re, q_im = ratio_re[g : g + 1], ratio_im[g : g + 1]
            d_re = q_re * b_re[n, g] - q_im * b_im[n, g]
            d_im = q_re * b_im[n, g] + q_im * b_re[n, g]
            drives.append(jnp.concatenate([d_re, d_im], axis=1))
            reads.append(jnp.concatenate([r_re[n, g], -r_im[n, g]], axis=1))
            k_re, k_im = keep_re[g : g + 1], keep_im[g : g + 1]
            old = state[n, :, g, :]
            swapped = jnp.concatenate([old[:, half:], old[:, :half]], axis=1)
            new = (
                jnp.concatenate([k_re, k_re], axis=1) * old
                + jnp.concatenate([-k_im, k_im], axis=1) * swapped
            )
            base[n, :, g, :] = new
            offsets.append(times_turned(new, reads[g], HIGHEST))
        dcat = jnp.concatenate(drives)
        spread = []
        for g in range(groups):
            zero = jnp.zeros_like(drives[g])
            spread.append(jnp.concatenate([drives[g] if h == g else zero for h in range(groups)], axis=1))
        drive_high[n], drive_low[n] = two_halves(jnp.concatenate(spread))
        full = times_turned(dcat, jnp.concatenate(reads), HIGHEST)
        mix = jnp.where(row // chans == col // chans, full, 0.0)
        mix = mix + jnp.where(row == col, d_skip[n : n + 1, :], 0.0)
        carried[n * SEQS : (n + 1) * SEQS, :] = jnp.concatenate(offsets, axis=1)
        compact = mix[:chans]
        for g in range(1, groups):
            compact = compact + mix[g * chans : (g + 1) * chans]
        top = LAYERS * SEQS + n * chans
        carried[top : top + chans, :] = compact


def write_payload(pay_ref, x, blocks, carried, n):
    squares = jnp.sum(x * x, axis=1, keepdims=True)
    s_high, s_low = two_halves(squares)
    lane = lax.broadcasted_iota(jnp.int32, (SEQS, BLOCK), 1)
    s_part = jnp.where(lane == 0, s_high.astype(f32), jnp.where(lane == 1, s_low.astype(f32), 0.0))
    top = LAYERS * SEQS + n * CHANS
    row = jnp.concatenate(
        [blocks[j].astype(bf16) for j in range(NZ)]
        + [*two_halves(carried[n * SEQS : (n + 1) * SEQS])]
        + [jnp.concatenate(two_halves(carried[top : top + CHANS])), s_part.astype(bf16)],
        axis=1,
    )
    for i in range(ND):
        pay_ref[i] = row


def times_turned(left, right, precision=None):
    return lax.dot_general(
        left, right, (((1,), (1,)), ((), ())), precision=precision, preferred_element_type=f32
    )


def first_kernel(p0, p1, p2, p3, gain, carried, w, pay_ref, x_ref, rows):
    y = lax.axis_index("y")
    for k, piece in enumerate((p0, p1, p2, p3)):
        rows[lax.rem(y + NY - k, NY)] = piece[...].astype(f32)
    x = rows[...].reshape(SEQS, COLS)
    x_ref[...] = x
    normed = (x * gain[0:1]).astype(bf16)
    blocks = [times_turned(normed, w[j]) for j in range(NZ)]
    write_payload(pay_ref, x, blocks, carried, 0)


def next_kernel(out, r1, r2, r3, x_old, gain, carried, *refs):
    w = refs[:NZ]
    pay_ref, x_ref, blocks = refs[NZ:]
    z = lax.axis_index("z")
    total = out[...] + r1[...] + r2[...] + r3[...]
    x = x_old[...] + total[:, :COLS] * jax.nn.sigmoid(total[:, COLS:])
    x = x.astype(bf16).astype(f32)
    x_ref[...] = x
    normed = (x * gain[1:2]).astype(bf16)
    for k in range(NZ):
        blocks[lax.rem(z + NZ - k, NZ)] = times_turned(normed, w[k][:, 2 * COLS : 3 * COLS])
    write_payload(pay_ref, x, blocks, carried, 1)


def inputs_of(got):
    total = got[0, :, :WIDTH].astype(f32)
    squares = got[0, :, WIDTH + 192 :].astype(f32)
    for i in range(1, ND):
        total = total + got[i, :, :WIDTH].astype(f32)
        squares = squares + got[i, :, WIDTH + 192 :].astype(f32)
    return total * lax.rsqrt(jnp.sum(squares, axis=1, keepdims=True) / D + eps)


def gated(got, u_blocks, w, ordered, weights):
    z = lax.axis_index("z")
    row = lax.broadcasted_iota(jnp.int32, (BLOCK, BLOCK), 0)
    col = lax.broadcasted_iota(jnp.int32, (BLOCK, BLOCK), 1)
    same = row // CHANS == col // CHANS
    for delta in range(NZ):
        block, slot, source = lax.rem(z + delta, NZ), (NZ - delta) % NZ, place(z, delta)
        sent = got[source]
        offset = sent[:, WIDTH : WIDTH + BLOCK].astype(f32)
        offset = offset + sent[:, WIDTH + BLOCK : WIDTH + 2 * BLOCK].astype(f32)
        cut = slice(slot * BLOCK, (slot + 1) * BLOCK)
        weights[cut, :] = w[slot][:, : 2 * COLS]
        m = sent[:, WIDTH + 128 : WIDTH + 192].astype(f32)
        m_high = jnp.where(same, jnp.concatenate([m[:CHANS]] * (BLOCK // CHANS)), 0.0).astype(bf16)
        m_low = jnp.where(same, jnp.concatenate([m[CHANS:]] * (BLOCK // CHANS)), 0.0).astype(bf16)
        high, low = two_halves(u_blocks[block])
        pre = (
            offset
            + jnp.dot(high, m_low, preferred_element_type=f32)
            + jnp.dot(low, m_high, preferred_element_type=f32)
            + jnp.dot(high, m_high, preferred_element_type=f32)
        )
        ordered[:, cut] = jax.nn.gelu(pre).astype(bf16)
    return jnp.dot(ordered[...], weights[...], preferred_element_type=f32)


def own_block(u_blocks):
    z = lax.axis_index("z")
    d = lax.axis_index("x") * NC + lax.axis_index("c")
    delta = jnp.int32(0)
    for other in range(1, NZ):
        delta = jnp.where(place(z, other) == d, other, delta)
    return u_blocks[lax.rem(z + delta, NZ)]


def split_blocks(u, u_blocks):
    for j in range(NZ):
        u_blocks[j] = u[:, j * BLOCK : (j + 1) * BLOCK]


def mid_kernel(got, *refs):
    w = refs[:NZ]
    out, own_u, u_blocks, ordered, weights = refs[NZ:]
    split_blocks(inputs_of(got), u_blocks)
    own_u[...] = own_block(u_blocks)
    out[...] = gated(got, u_blocks, w, ordered, weights)


def inputs_kernel(got, earlier, u_blocks, own_u):
    split_blocks(inputs_of(got), u_blocks)
    own_u[:SEQS, :] = earlier[...]
    own_u[SEQS:, :] = own_block(u_blocks)


def last_kernel(got, u_blocks, *refs):
    w = refs[:NZ]
    own_out, s1, s2, s3, ordered, weights, by_y = refs[NZ:]
    out = gated(got, u_blocks, w, ordered, weights)
    y = lax.axis_index("y")
    by_y[...] = out.reshape(NY, ROWS, 2 * COLS)
    own_out[...] = by_y[y]
    for k, ref in enumerate((s1, s2, s3), 1):
        ref[...] = by_y[lax.rem(y + k, NY)]


def stream_kernel(own, r1, r2, r3, x, out):
    y = lax.axis_index("y")
    total = own[...] + r1[...] + r2[...] + r3[...]
    mine = x[pl.ds(pl.multiple_of(y * ROWS, ROWS), ROWS), :]
    out[...] = (mine + total[:, :COLS] * jax.nn.sigmoid(total[:, COLS:])).astype(bf16)


def states_kernel(base, drive_high, drive_low, u, out):
    groups, doubled = base.shape[2:]
    for n in range(LAYERS):
        high, low = two_halves(u[n * SEQS : (n + 1) * SEQS, :])
        push = (
            jnp.dot(high, drive_low[n], preferred_element_type=f32)
            + jnp.dot(low, drive_high[n], preferred_element_type=f32)
            + jnp.dot(high, drive_high[n], preferred_element_type=f32)
        )
        for g in range(groups):
            out[n, :, g, :] = base[n, :, g, :] + push[:, g * doubled : (g + 1) * doubled]


def call(body, args, outs, scratch=(), scalar=None, space=pltpu.VMEM):
    spaces = [pltpu.SMEM if i == scalar else space for i in range(len(args))]
    return pl.pallas_call(
        body,
        in_specs=[pl.BlockSpec(memory_space=s) for s in spaces],
        out_specs=[pl.BlockSpec(memory_space=pltpu.VMEM) for _ in outs],
        out_shape=outs,
        scratch_shapes=list(scratch),
        compiler_params=pltpu.CompilerParams(vmem_limit_bytes=(60 if space is pl.ANY else 12) << 20),
        cost_estimate=pl.CostEstimate(flops=1 << 24, bytes_accessed=1 << 20, transcendentals=0),
    )(*args)


def shape(dims, dtype=f32):
    return jax.ShapeDtypeStruct(dims, dtype)


PAY_OUTS = [shape((ND, SEQS, WIDTH + 256), bf16), shape((SEQS, COLS))]
BLOCKS = pltpu.VMEM((NZ, SEQS, BLOCK), f32)
GATED = [pltpu.VMEM((SEQS, WIDTH), bf16), pltpu.VMEM((WIDTH, 2 * COLS), bf16)]


def both_layers(
    stream,
    norm_gain,
    w_input,
    lam_re,
    lam_im,
    log_dt,
    b_re,
    b_im,
    readout_real,
    readout_imaginary,
    d_skip,
    w_val,
    w_gate,
    state,
):
    w_turned = jnp.swapaxes(w_input, 1, 2)
    packed, soon, late = call(
        pack_kernel,
        [w_turned, w_val, w_gate],
        [
            shape((NZ, BLOCK, COLS), bf16),
            shape((BLOCK, 3 * COLS), bf16),
            shape((BLOCK, 2 * COLS), bf16),
        ],
        [
            pltpu.VMEM((BLOCK, COLS), bf16),
            pltpu.VMEM((BLOCK, 3 * COLS), bf16),
            pltpu.VMEM((BLOCK, 2 * COLS), bf16),
            pltpu.SemaphoreType.DMA((6,)),
        ],
        space=pl.ANY,
    )
    first_w = lax.all_to_all(packed, "z", 0, 0, tiled=True)
    after = shift_y(stream, 1)
    before = shift_y(stream, -1)
    pieces = [stream, after, shift_y(after, 1), before]
    base, drive_high, drive_low, own = call(
        prep_kernel,
        [
            lam_re,
            lam_im,
            log_dt,
            jnp.swapaxes(b_re, 2, 3),
            jnp.swapaxes(b_im, 2, 3),
            readout_real,
            readout_imaginary,
            d_skip,
            state,
        ],
        [
            shape(state.shape),
            shape((LAYERS, BLOCK, 2 * COLS), bf16),
            shape((LAYERS, BLOCK, 2 * COLS), bf16),
            shape((LAYERS * (SEQS + CHANS), BLOCK)),
        ],
        scalar=2,
    )
    carried = turn(own)
    ring_soon = ring_z(soon)
    ring_late = ring_z(late)

    payload, x = call(
        first_kernel,
        [*pieces, norm_gain, carried, first_w],
        PAY_OUTS,
        [pltpu.VMEM((NY, ROWS, COLS), f32)],
    )
    got = lax.all_to_all(payload, DP, 0, 0, tiled=True)
    out, u0 = call(
        mid_kernel,
        [got, *ring_soon],
        [shape((SEQS, 2 * COLS)), shape((SEQS, BLOCK))],
        [BLOCKS, *GATED],
    )
    others = [shift_y(out, k) for k in range(1, NY)]
    payload, x = call(
        next_kernel,
        [out, *others, x, norm_gain, carried, *ring_soon],
        PAY_OUTS,
        [BLOCKS],
    )
    got = lax.all_to_all(payload, DP, 0, 0, tiled=True)
    u, both = call(
        inputs_kernel, [got, u0], [shape((NZ, SEQS, BLOCK)), shape((LAYERS * SEQS, BLOCK))]
    )
    both = turn(both, back=True)
    own, s1, s2, s3 = call(
        last_kernel,
        [got, u, *ring_late],
        [shape((ROWS, 2 * COLS))] * NY,
        [*GATED, pltpu.VMEM((NY, ROWS, 2 * COLS), f32)],
    )
    others = [shift_y(sent, k) for k, sent in enumerate((s1, s2, s3), 1)]
    (stream,) = call(stream_kernel, [own, *others, x], [shape((ROWS, COLS), bf16)])
    (states,) = call(states_kernel, [base, drive_high, drive_low, both], [shape(state.shape)])
    return (stream, states)


def solution(mesh):
    grid = Mesh(mesh.devices.reshape(NZ, NY, NX, NC), ALL)
    return jax.shard_map(
        both_layers,
        mesh=grid,
        in_specs=(
            P(TP, DP),
            P(None, DP),
            P(None, DP, TP),
            P(None, TP, None),
            P(None, TP, None),
            P(None, TP),
            P(None, TP, None, None),
            P(None, TP, None, None),
            P(None, TP, None, None),
            P(None, TP, None, None),
            P(None, TP),
            P(None, TP, DP),
            P(None, TP, DP),
            P(None, DP, TP, None),
        ),
        out_specs=(P(TP, DP), P(None, DP, TP, None)),
        check_vma=False,
    )
```
